256 devices in a mesh: sp: 64 (over z, y, core), tp: 4 (over x).
Axes of the slice: x: 4, y: 4, z: 8, core: 2. Of those that a mesh axis runs over, the one named last changes fastest.
Arguments:
- memory_queries: bfloat16 [32768, 1024], P('sp', 'tp'), may hold values from -8 to 8
- memory_keys: bfloat16 [32768, 1024], P('sp', 'tp'), may hold values from -8 to 8
- memory_values: bfloat16 [32768, 1024], P('sp', 'tp'), may hold values from -6 to 6
- input_gate_logits: float32 [8, 32768], P('tp', 'sp'), may hold values from -64 to 160
- forget_gate_logits: float32 [8, 32768], P('tp', 'sp'), may hold values from -0.1 to 20
- extra_log_decay: float32 [8, 32768], P('tp', 'sp'), may hold values from -1.4 to 0
- residual: bfloat16 [32768, 2048], P(('sp', 'tp')), may hold values from -6 to 6
- cell_output_weight: bfloat16 [1024, 2048], P('tp', 'sp'), may hold values from -0.1875 to 0.1875
- expert_norm_gain: float32 [2048], replicated, may hold values from 0.1 to 1.9
- expert_gate_weight: bfloat16 [64, 2048, 3584], P('sp', None, 'tp'), may hold values from -0.125 to 0.125
- expert_up_weight: bfloat16 [64, 2048, 3584], P('sp', None, 'tp'), may hold values from -0.125 to 0.125
- expert_down_weight: bfloat16 [64, 3584, 2048], P('sp', 'tp'), may hold values from -0.09375 to 0.09375
- routed_expert_index: int32 [32768, 2], P('sp'), may hold values from 0 to 63, as said below
- routed_expert_weight: float32 [32768, 2], P(('sp', 'tp')), may hold values from 0.1 to 1
Outputs:
- layer_out: bfloat16 [32768, 2048], P(('sp', 'tp'))
The draws below stay inside these ranges and needn't reach their ends.
Inputs may be any that keep to these rules, and one draw needn't show every extreme that they name: `routed_expert_index`: each row names 2 different experts. In each aligned block of 128 rows (the rows of one device after the cell) no expert is named more than 5 times, and one expert is named exactly 5 times in every block.
All inputs are finite; a program needn't handle non-finite values.
Results may differ from the reference program's by a relative error of at most 0.013.
Values may be sent and summed in bfloat16 or wider, within the bound.
No kernel may reach another device: no remote copies, remote signals or barrier semaphores. Data moves between devices by JAX's collectives and lax.ppermute only.
A program may use at most 128 MiB of HBM per device.

```python
import math
import jax
import jax.numpy as jnp
from jax import lax

D = 2048
RECURRENT_LANES = 8
DH = 128
FF = 3584
TOPK = 2
TOK_DEV = 512
TEXT_LENGTH = 32768
ROWS = 128
HD = 1024
EXPERTS = 64
CAP = 5
EXPERT_ROWS = 1280
N_TP = 4


def shared_direction(key):
    return jnp.clip(jax.random.normal(jax.random.fold_in(key, 3), (RECURRENT_LANES * DH,), jnp.float32), -4.0, 4.0)


def query_like(key, salt_id):
    offset = 0.95
    dims_all = (TEXT_LENGTH, RECURRENT_LANES * DH)
    jitter = jnp.clip(jax.random.normal(jax.random.fold_in(key, salt_id), dims_all, jnp.float32), -4.0, 4.0)
    return jitter + offset * shared_direction(key)[None, :]


def draw_memory_queries(key, part):
    return query_like(key, 5).astype(jnp.bfloat16)


def draw_memory_keys(key, part):
    return query_like(key, 6).astype(jnp.bfloat16)


def draw_input_gate_logits(key, part):
    dims_all = (RECURRENT_LANES, TEXT_LENGTH)
    return 2.5 * jnp.clip(jax.random.normal(jax.random.fold_in(key, 8), dims_all, jnp.float32), -4.0, 4.0)


def draw_forget_gate_logits(key, part):
    ranking = jax.random.permutation(jax.random.fold_in(key, 12), RECURRENT_LANES)
    quick_count = RECURRENT_LANES // 2
    center = jnp.where(ranking < quick_count, math.log(40.0), math.log(TEXT_LENGTH) + 1.5).astype(jnp.float32)
    device_shift = jax.random.uniform(jax.random.fold_in(key, 13), (TEXT_LENGTH // TOK_DEV,), jnp.float32, -0.7, 0.7)
    device_shift = jnp.repeat(device_shift, TOK_DEV)
    jitter = jnp.clip(jax.random.normal(jax.random.fold_in(key, 14), (RECURRENT_LANES, TEXT_LENGTH), jnp.float32), -3.0, 3.0)
    return center[:, None] + device_shift[None, :] + jitter


def draw_extra_log_decay(key, part):
    surge_offset = jax.random.randint(jax.random.fold_in(key, 15), (RECURRENT_LANES, 3, 1), 0, TEXT_LENGTH)
    element_levels = jax.random.uniform(jax.random.fold_in(key, 16), (RECURRENT_LANES, 3, 1), jnp.float32, -0.69, -0.22)
    seat_locations = jnp.arange(TEXT_LENGTH)[None, None, :]
    return jnp.sum(jnp.where(seat_locations == surge_offset, element_levels, 0.0), axis=1)


def draw_routed_expert_index(key, part):
    specialist_capacity = EXPERTS * CAP
    assigned = ROWS * TOPK
    specialist_table = jnp.arange(specialist_capacity) // CAP
    favour_increment = jax.random.randint(jax.random.fold_in(key, 21), (EXPERTS,), 0, 3) * 4096
    chosen_specialists = jax.random.randint(jax.random.fold_in(key, 22), (), 0, EXPERTS)
    additional_reward = favour_increment[specialist_table] + jnp.where(specialist_table == chosen_specialists, 16384, 0)

    def one_block(address_tile_range):
        dispatch_affinity = jax.random.randint(jax.random.fold_in(address_tile_range, 1), (specialist_capacity,), 0, 4096) + additional_reward
        ranked = dispatch_affinity * specialist_capacity + jnp.arange(specialist_capacity)
        picked = lax.top_k(ranked, assigned)[1]
        names = jnp.sort(specialist_table[picked]).reshape(TOPK, ROWS).T
        turn = jax.random.randint(jax.random.fold_in(address_tile_range, 2), (ROWS, 1), 0, TOPK)
        names = jnp.take_along_axis(names, (jnp.arange(TOPK)[None, :] + turn) % TOPK, axis=1)
        return names[jax.random.permutation(jax.random.fold_in(address_tile_range, 3), ROWS)]
    block_keys = jax.random.split(jax.random.fold_in(key, 23), TEXT_LENGTH // ROWS)
    return jax.vmap(one_block)(block_keys).reshape(TEXT_LENGTH, TOPK).astype(jnp.int32)


def level_of(own_key, shape, cuts, smallest, largest):
    level = 1.0
    for axis_at, shards_of in cuts:
        draws = jax.random.uniform(jax.random.fold_in(jax.random.fold_in(own_key, 6), axis_at), (shards_of,), jnp.float32, smallest / len(cuts), largest / len(cuts))
        level = level * jnp.repeat(jnp.exp(draws), shape[axis_at] // shards_of).reshape((-1,) + (1,) * (len(shape) - 1 - axis_at))
    return level


def gaussian(rng, dims, scale, bound, shards=(), held_as=jnp.bfloat16):
    drawn = jax.random.normal(rng, dims, jnp.float32) * scale
    if len(shards) > 0:
        drawn = level_of(rng, dims, shards, -0.22, 0.18) * drawn
    return jnp.clip(drawn, min=-bound, max=bound).astype(held_as)


def setup_inputs(seed: int = 0) -> dict:
    key_list = jax.random.split(jax.random.key(seed), 15)
    return {
        "memory_queries": draw_memory_queries(jax.random.fold_in(key_list[14], 71), 0),
        "memory_keys": draw_memory_keys(jax.random.fold_in(key_list[14], 71), 0),
        "memory_values": gaussian(key_list[2], (TEXT_LENGTH, HD), 1.0, 6.0, ((0, 64), (1, 4))),
        "input_gate_logits": draw_input_gate_logits(jax.random.fold_in(key_list[14], 71), 0),
        "forget_gate_logits": draw_forget_gate_logits(jax.random.fold_in(key_list[14], 71), 0),
        "extra_log_decay": draw_extra_log_decay(jax.random.fold_in(key_list[14], 71), 0),
        "residual": gaussian(key_list[6], (TEXT_LENGTH, D), 1.0, 6.0, ((0, 256),)),
        "cell_output_weight": gaussian(key_list[7], (HD, D), HD ** -0.5, 0.1875, ((0, 4), (1, 64))),
        "expert_norm_gain": jnp.clip(1.0 + 0.18 * jax.random.normal(key_list[8], (D,), jnp.float32), 0.1, 1.9),
        "expert_gate_weight": gaussian(key_list[9], (EXPERTS, D, FF), D ** -0.5, 0.125, ((0, 64), (2, 4))),
        "expert_up_weight": gaussian(key_list[10], (EXPERTS, D, FF), D ** -0.5, 0.125, ((0, 64), (2, 4))),
        "expert_down_weight": gaussian(key_list[11], (EXPERTS, FF, D), FF ** -0.5, 0.09375, ((0, 64), (1, 4))),
        "routed_expert_index": draw_routed_expert_index(jax.random.fold_in(key_list[14], 71), 0),
        "routed_expert_weight": jnp.clip(0.1 + 0.9 * jax.random.uniform(key_list[13], (TEXT_LENGTH, TOPK), jnp.float32) ** level_of(key_list[13], (TEXT_LENGTH, TOPK), ((0, 256),), -0.2, 0.2), 0.1, 1.0),
    }


highest = lax.Precision.HIGHEST
lowest = -1e+30
epsilon = 1e-06

def block_pass(memory, inputs):
    state_mat, state_norm, state_max = memory
    queries, keys_blk, values_blk, gate_in, forget_log_value = inputs
    length = gate_in.shape[-1]
    running = jnp.cumsum(forget_log_value, axis=-1)
    causal = jnp.arange(length)[:, None] >= jnp.arange(length)[None, :]
    exponent = running[:, :, None] - running[:, None, :] + gate_in[:, None, :]
    exponent = jnp.where(causal[None], exponent, -jnp.inf)
    carried = running + state_max[:, None]
    row_max = jnp.maximum(carried, lax.optimization_barrier(jnp.max(exponent, axis=-1)))
    decays = jnp.exp(exponent - row_max[:, :, None])
    carry_scale = jnp.exp(carried - row_max)
    dispatch_affinity = jnp.einsum('htk,hsk->hts', queries, keys_blk, precision=highest) * decays
    numerator = carry_scale[:, :, None] * jnp.einsum('hvk,htk->htv', state_mat, queries, precision=highest)
    numerator = numerator + jnp.einsum('hts,hsv->htv', dispatch_affinity, values_blk, precision=highest)
    denominator = carry_scale * jnp.einsum('hk,htk->ht', state_norm, queries, precision=highest) + lax.optimization_barrier(jnp.sum(dispatch_affinity, axis=-1))
    final_log = running[:, -1]
    log_prev = final_log + state_max
    log_keep = final_log[:, None] - running + gate_in
    new_max = jnp.maximum(log_prev, lax.optimization_barrier(jnp.max(log_keep, axis=-1)))
    prev_scale = jnp.exp(log_prev - new_max)
    retain = jnp.exp(log_keep - new_max[:, None])
    new_mat = prev_scale[:, None, None] * state_mat + jnp.einsum('hsv,hsk->hvk', retain[:, :, None] * values_blk, keys_blk, precision=highest)
    new_norm = prev_scale[:, None] * state_norm + jnp.einsum('hs,hsk->hk', retain, keys_blk, precision=highest)
    output = numerator / jnp.maximum(jnp.abs(denominator), jnp.exp(-row_max))[:, :, None]
    return ((new_mat, new_norm, new_max), output)

def heads_first(tensor):
    return jnp.transpose(tensor.astype(jnp.float32).reshape(TEXT_LENGTH, RECURRENT_LANES, DH), (1, 0, 2))

def reference(memory_queries, memory_keys, memory_values, input_gate_logits, forget_gate_logits, extra_log_decay, residual, cell_output_weight, expert_norm_gain, expert_gate_weight, expert_up_weight, expert_down_weight, routed_expert_index, routed_expert_weight):
    block_size = min(TOK_DEV, 256)
    block_count = TEXT_LENGTH // block_size

    def split_blocks(tensor):
        return jnp.moveaxis(tensor.reshape((RECURRENT_LANES, block_count, block_size) + tensor.shape[2:]), 1, 0)
    queries = heads_first(memory_queries) * DH ** (-0.5)
    forget_log_value = jax.nn.log_sigmoid(forget_gate_logits) + extra_log_decay
    start_state = (jnp.zeros((RECURRENT_LANES, DH, DH), jnp.float32), jnp.zeros((RECURRENT_LANES, DH), jnp.float32), jnp.full((RECURRENT_LANES,), lowest, jnp.float32))
    members = (queries, heads_first(memory_keys), heads_first(memory_values), input_gate_logits, forget_log_value)
    end_state, outputs = lax.scan(block_pass, start_state, tuple((split_blocks(member) for member in members)))
    hidden = jnp.moveaxis(outputs, 0, 1).reshape(RECURRENT_LANES, TEXT_LENGTH, DH).astype(jnp.bfloat16)
    flat_hidden = jnp.transpose(hidden, (1, 0, 2)).reshape(TEXT_LENGTH, HD)
    quarter = HD // N_TP
    projected = jnp.zeros((TEXT_LENGTH, D), jnp.float32)
    for owner_idx in range(N_TP):
        low_col = owner_idx * quarter
        group_term = jnp.dot(flat_hidden[:, low_col:low_col + quarter], cell_output_weight[low_col:low_col + quarter], preferred_element_type=jnp.float32)
        projected = projected + lax.optimization_barrier(group_term.astype(jnp.bfloat16)).astype(jnp.float32)
    mixed_rows = (residual.astype(jnp.float32) + projected).astype(jnp.bfloat16)
    mixed_wide = mixed_rows.astype(jnp.float32)
    norm_scale = lax.rsqrt(lax.optimization_barrier(jnp.mean(mixed_wide * mixed_wide, axis=-1, keepdims=True)) + epsilon)
    normed = (mixed_wide * norm_scale * expert_norm_gain).astype(jnp.bfloat16)
    normed_pad = jnp.concatenate([normed, jnp.zeros((1, D), jnp.bfloat16)], axis=0)
    hidden_part = FF // N_TP

    def one_expert(running_sum, expert):
        matched = routed_expert_index == expert
        weight_tok = jnp.concatenate([lax.optimization_barrier(jnp.sum(jnp.where(matched, routed_expert_weight, 0.0), axis=1)), jnp.zeros((1,), jnp.float32)])
        picked = jnp.nonzero(jnp.any(matched, axis=1), size=EXPERT_ROWS, fill_value=TEXT_LENGTH)[0]
        rows_in = normed_pad[picked]
        gate_all = expert_gate_weight[expert]
        up_all = expert_up_weight[expert]
        down_all = expert_down_weight[expert]
        result = jnp.zeros((EXPERT_ROWS, D), jnp.float32)
        for owner_idx in range(N_TP):
            low_col = owner_idx * hidden_part
            gate_pre = jnp.dot(rows_in, gate_all[:, low_col:low_col + hidden_part], preferred_element_type=jnp.float32)
            up_pre = jnp.dot(rows_in, up_all[:, low_col:low_col + hidden_part], preferred_element_type=jnp.float32)
            hidden_act = (jax.nn.silu(gate_pre) * up_pre).astype(jnp.bfloat16)
            group_term = jnp.dot(hidden_act, down_all[low_col:low_col + hidden_part], preferred_element_type=jnp.float32)
            result = result + lax.optimization_barrier(group_term.astype(jnp.bfloat16)).astype(jnp.float32)
        returned = lax.optimization_barrier(result.astype(jnp.bfloat16)).astype(jnp.float32)
        return (running_sum.at[picked].add(returned * weight_tok[picked][:, None], mode='drop'), None)
    routed, _ = lax.scan(one_expert, jnp.zeros((TEXT_LENGTH, D), jnp.float32), jnp.arange(EXPERTS, dtype=jnp.int32))
    return (mixed_wide + routed).astype(jnp.bfloat16)
```

```python
import jax
import jax.numpy as jnp
from jax import lax
from jax.experimental import pallas as pl
from jax.experimental.pallas import tpu as pltpu
from jax.sharding import Mesh
from jax.sharding import PartitionSpec as P

SP = ("sp_0", "sp_1", "sp_2")
SP_TP = ("sp_0", "sp_1", "sp_2", "tp")


lowest = -1e30
epsilon = 1e-06


def sent_round(x, axis):
    return lax.all_to_all(x, axis, split_axis=0, concat_axis=0, tiled=True)


def shifted(x, axis, by):
    size = lax.axis_size(axis)
    return lax.ppermute(x, axis, [(i, (i + by) % size) for i in range(size)])


def earlier_state(final_log, mat, norm, peak):
    size, heads = lax.axis_size(SP), final_log.shape[0]
    width = mat.shape[-1]
    per_slice = norm.size // size
    side = jnp.concatenate(
        [
            norm.reshape(size, per_slice),
            jnp.broadcast_to(final_log, (size, heads)),
            jnp.broadcast_to(peak, (size, heads)),
        ],
        axis=1,
    )
    side = jnp.pad(side, ((0, 0), (0, width - side.shape[1])))[:, None, :]
    body = mat.reshape(size, -1, width)
    rows = body.shape[1]
    sent = jnp.concatenate([body, side], axis=1)
    sent = jnp.pad(sent, ((0, 0), (0, -sent.shape[1] % 8), (0, 0)))
    got = sent_round(sent, SP)
    head = lax.axis_index(SP) * heads // size
    logs = got[:, rows, per_slice : per_slice + heads]
    peaks = got[:, rows, per_slice + heads : per_slice + 2 * heads]
    mine = jnp.arange(heads)[None, :] == head
    logs = jnp.sum(jnp.where(mine, logs, 0.0), axis=1)
    peaks = jnp.sum(jnp.where(mine, peaks, 0.0), axis=1)
    spot = jnp.arange(size)
    between = (spot[None, None, :] < spot[:, None, None]) & (
        spot[None, None, :] > spot[None, :, None]
    )
    decay = jnp.sum(jnp.where(between, logs[None, None, :], 0.0), axis=-1)
    before = spot[None, :] < spot[:, None]
    level = jnp.where(before, peaks[None, :] + decay, lowest)
    top = jnp.max(level, axis=1)
    scale = jnp.where(before, jnp.exp(level - top[:, None]), 0.0)
    joined = jnp.dot(
        scale, got.reshape(size, -1), precision=lax.Precision.HIGHEST
    ).reshape(got.shape)
    spread = (jnp.arange(got.shape[1])[:, None] == rows) & (
        jnp.arange(width)[None, :] == per_slice
    )
    joined = jnp.where(spread[None], top[:, None, None], joined)
    back = sent_round(joined, SP)
    prior_mat = back[:, :rows].reshape(mat.shape)
    prior_norm = back[:, rows, :per_slice].reshape(norm.shape)
    prior_peak = back[:: size // heads, rows, per_slice]
    return prior_mat, prior_norm, prior_peak


def ring_gathered(first, second, axis):
    left_1 = shifted(first, axis, 1)
    right_2 = shifted(second, axis, -1)
    left_2 = shifted(second, axis, 1)
    right_1 = shifted(first, axis, -1)
    far_1 = shifted(left_1, axis, 1)
    far_2 = shifted(right_2, axis, -1)
    return (first, second, left_1, left_2, right_1, right_2, far_1, far_2)


def wide(x):
    return x.astype(jnp.float32)


def ring_summed(blocks, axis):
    own_1, own_2, left_1, left_2, right_1, right_2, far_1, far_2 = blocks
    far_in_1 = shifted(far_1, axis, 1)
    far_in_2 = shifted(far_2, axis, -1)
    from_left_2 = shifted(right_2, axis, 1)
    from_right_1 = shifted(left_1, axis, -1)
    from_left_1 = shifted((wide(right_1) + wide(far_in_1)).astype(jnp.bfloat16), axis, 1)
    from_right_2 = shifted((wide(left_2) + wide(far_in_2)).astype(jnp.bfloat16), axis, -1)
    first = wide(own_1) + wide(from_left_1) + wide(from_right_1)
    second = wide(own_2) + wide(from_left_2) + wide(from_right_2)
    return first, second


def expert_kernel(count, rows, *refs):
    given, (gate_hbm, up_hbm, down_hbm) = refs[:count], refs[count : count + 3]
    outs = refs[count + 3 : 2 * count + 3]
    rows_in, rows_out, gate, up, down, in_sems, w_sems, out_sems = refs[2 * count + 3 :]
    copies = []
    for k in range(count):
        copies.append(
            pltpu.make_async_copy(given[k], rows_in.at[pl.ds(k * rows, rows)], in_sems.at[k])
        )
    loads = [
        pltpu.make_async_copy(gate_hbm, gate, w_sems.at[0]),
        pltpu.make_async_copy(up_hbm, up, w_sems.at[1]),
        pltpu.make_async_copy(down_hbm, down, w_sems.at[2]),
    ]
    loads[0].start()
    for copy in copies:
        copy.start()
    loads[1].start()
    loads[2].start()
    for copy in copies:
        copy.wait()
    for load in loads:
        load.wait()
    tile = count * rows // 2

    def one_tile(k, carry):
        here = pl.ds(pl.multiple_of(k * tile, tile), tile)
        x = rows_in[here, :]
        gate_pre = jnp.dot(x, gate[...], preferred_element_type=jnp.float32)
        up_pre = jnp.dot(x, up[...], preferred_element_type=jnp.float32)
        inner = (gate_pre / (1.0 + jnp.exp(-gate_pre)) * up_pre).astype(jnp.bfloat16)
        rows_out[here, :] = jnp.dot(
            inner, down[...], preferred_element_type=jnp.float32
        ).astype(jnp.bfloat16)
        return carry

    lax.fori_loop(0, 2, one_tile, 0)
    stores = []
    for k in range(count):
        stores.append(
            pltpu.make_async_copy(rows_out.at[pl.ds(k * rows, rows)], outs[k], out_sems.at[k])
        )
    for store in stores:
        store.start()
    for store in stores:
        store.wait()


def expert_rows(blocks, gate_weight, up_weight, down_weight):
    count = len(blocks)
    rows, width = blocks[0].shape
    hidden = gate_weight.shape[1]
    anywhere = pl.BlockSpec(memory_space=pl.ANY)
    flops = 6 * count * rows * width * hidden
    return pl.pallas_call(
        lambda *refs: expert_kernel(count, rows, *refs),
        out_shape=[jax.ShapeDtypeStruct((rows, width), jnp.bfloat16)] * count,
        in_specs=[anywhere] * (count + 3),
        out_specs=[anywhere] * count,
        scratch_shapes=[
            pltpu.VMEM((count * rows, width), jnp.bfloat16),
            pltpu.VMEM((count * rows, width), jnp.bfloat16),
            pltpu.VMEM((width, hidden), jnp.bfloat16),
            pltpu.VMEM((width, hidden), jnp.bfloat16),
            pltpu.VMEM((hidden, width), jnp.bfloat16),
            pltpu.SemaphoreType.DMA((count,)),
            pltpu.SemaphoreType.DMA((3,)),
            pltpu.SemaphoreType.DMA((count,)),
        ],
        compiler_params=pltpu.CompilerParams(vmem_limit_bytes=40 * 1024 * 1024),
        cost_estimate=pl.CostEstimate(
            flops=flops,
            transcendentals=count * rows * hidden,
            bytes_accessed=6 * width * hidden + 4 * count * rows * width,
        ),
        name="expert_rows",
    )(*blocks, gate_weight, up_weight, down_weight)


def block_pass(memory, inputs):
    state_mat, state_norm, state_max = memory
    queries, keys_blk, values_blk, gate_in, forget_log_value = inputs
    length = gate_in.shape[-1]
    running = jnp.cumsum(forget_log_value, axis=-1)
    causal = jnp.arange(length)[:, None] >= jnp.arange(length)[None, :]
    exponent = running[:, :, None] - running[:, None, :] + gate_in[:, None, :]
    exponent = jnp.where(causal[None], exponent, -jnp.inf)
    carried = running + state_max[:, None]
    row_max = jnp.maximum(carried, jnp.max(exponent, axis=-1))
    decays = jnp.exp(exponent - row_max[:, :, None])
    carry_scale = jnp.exp(carried - row_max)
    dispatch_affinity = jnp.einsum("htk,hsk->hts", queries, keys_blk) * decays
    numerator = carry_scale[:, :, None] * jnp.einsum("hvk,htk->htv", state_mat, queries)
    numerator = numerator + jnp.einsum("hts,hsv->htv", dispatch_affinity, values_blk)
    denominator = carry_scale * jnp.einsum("hk,htk->ht", state_norm, queries) + jnp.sum(
        dispatch_affinity, axis=-1
    )
    final_log = running[:, -1]
    log_prev = final_log + state_max
    log_keep = final_log[:, None] - running + gate_in
    new_max = jnp.maximum(log_prev, jnp.max(log_keep, axis=-1))
    prev_scale = jnp.exp(log_prev - new_max)
    retain = jnp.exp(log_keep - new_max[:, None])
    new_mat = prev_scale[:, None, None] * state_mat + jnp.einsum(
        "hsv,hsk->hvk", retain[:, :, None] * values_blk, keys_blk
    )
    new_norm = prev_scale[:, None] * state_norm + jnp.einsum("hs,hsk->hk", retain, keys_blk)
    return ((new_mat, new_norm, new_max), (numerator, denominator, row_max))


def matrix_memory_step(
    memory_queries,
    memory_keys,
    memory_values,
    input_gate_logits,
    forget_gate_logits,
    extra_log_decay,
):
    tokens_here, channels = memory_queries.shape
    heads_here = input_gate_logits.shape[0]
    head_dim = channels // heads_here

    def heads_first(tensor):
        return jnp.transpose(
            tensor.astype(jnp.float32).reshape(tokens_here, heads_here, head_dim), (1, 0, 2)
        )

    queries = heads_first(memory_queries) * head_dim ** (-0.5)
    forget_log_value = jax.nn.log_sigmoid(forget_gate_logits) + extra_log_decay
    block_size = min(tokens_here, 256)
    block_count = tokens_here // block_size

    def split_blocks(tensor):
        return jnp.moveaxis(
            tensor.reshape((heads_here, block_count, block_size) + tensor.shape[2:]), 1, 0
        )

    def join_blocks(tensor):
        return jnp.moveaxis(tensor, 0, 1).reshape((heads_here, tokens_here) + tensor.shape[3:])

    empty_state = (
        jnp.zeros((heads_here, head_dim, head_dim), jnp.float32),
        jnp.zeros((heads_here, head_dim), jnp.float32),
        jnp.full((heads_here,), lowest, jnp.float32),
    )
    members = (
        queries,
        heads_first(memory_keys),
        heads_first(memory_values),
        input_gate_logits,
        forget_log_value,
    )
    end_state, pieces = lax.scan(
        block_pass, empty_state, tuple((split_blocks(member) for member in members))
    )
    numerator, denominator, row_max = (join_blocks(member) for member in pieces)
    running = jnp.cumsum(forget_log_value, axis=-1)
    prior_mat, prior_norm, prior_max = earlier_state(running[:, -1], *end_state)
    reached = running + prior_max[:, None]
    joined = jnp.maximum(row_max, reached)
    local_scale = jnp.exp(row_max - joined)
    carry_scale = jnp.exp(reached - joined)
    numerator = local_scale[:, :, None] * numerator + carry_scale[:, :, None] * jnp.einsum(
        "hvk,htk->htv", prior_mat, queries
    )
    denominator = local_scale * denominator + carry_scale * jnp.einsum(
        "hk,htk->ht", prior_norm, queries
    )
    guarded = jnp.maximum(jnp.abs(denominator), jnp.exp(-joined))
    return ((numerator / guarded[:, :, None]).astype(jnp.bfloat16), heads_here, head_dim)


def slot_index(ids, experts, capacity):
    flat_ids = ids.reshape(-1)
    matches = (flat_ids[:, None] == jnp.arange(experts, dtype=jnp.int32)[None, :]).astype(jnp.int32)
    before = jnp.cumsum(matches, axis=0) - matches
    return flat_ids * capacity + jnp.sum(before * matches, axis=1)


def local(
    memory_queries,
    memory_keys,
    memory_values,
    input_gate_logits,
    forget_gate_logits,
    extra_log_decay,
    residual,
    cell_output_weight,
    expert_norm_gain,
    expert_gate_weight,
    expert_up_weight,
    expert_down_weight,
    routed_expert_index,
    routed_expert_weight,
):
    hidden, heads_here, head_dim = matrix_memory_step(
        memory_queries,
        memory_keys,
        memory_values,
        input_gate_logits,
        forget_gate_logits,
        extra_log_decay,
    )
    weight_rows = sent_round(
        jnp.broadcast_to(cell_output_weight.T, (lax.axis_size(SP), *cell_output_weight.T.shape)), SP
    ).reshape(-1, cell_output_weight.shape[0])
    row_count, model_width = residual.shape
    place = lax.axis_index("tp")
    flat_hidden = jnp.transpose(hidden, (1, 0, 2)).reshape(hidden.shape[1], -1)
    half_rows = row_count // 2

    def part_rows(offset, half):
        start = (place + offset) % 4 * row_count + half * half_rows
        rows = lax.dynamic_slice_in_dim(flat_hidden, start, half_rows, 0)
        return lax.dot_general(
            rows, weight_rows, (((1,), (1,)), ((), ())), preferred_element_type=jnp.float32
        ).astype(jnp.bfloat16)

    shares = [part_rows(offset, half) for offset in (0, 3, 1, 2) for half in (0, 1)]
    projected = jnp.concatenate(ring_summed(shares, "tp"), axis=0)
    mixed_rows = (residual.astype(jnp.float32) + projected).astype(jnp.bfloat16)
    mixed_wide = mixed_rows.astype(jnp.float32)
    norm_scale = lax.rsqrt(jnp.mean(mixed_wide * mixed_wide, axis=-1, keepdims=True) + epsilon)
    normed = (mixed_wide * norm_scale * expert_norm_gain).astype(jnp.bfloat16)
    sp_size = lax.axis_size(SP)
    top_count = routed_expert_index.shape[1]
    experts = sp_size * expert_gate_weight.shape[0]
    assigned = row_count * top_count
    capacity = max(2, assigned * 5 // (4 * experts))
    own_ids = lax.dynamic_slice_in_dim(routed_expert_index, place * row_count, row_count, 0)
    own_slots = slot_index(own_ids, experts, capacity).reshape(row_count, top_count)
    routed_sum = jnp.zeros((row_count, model_width), jnp.float32)
    chunks = ((0, 3), (3, 5))
    lane = 128
    sub = model_width // lane
    arrived = []
    for low, high in chunks:
        slots = jnp.arange(experts)[:, None] * capacity + jnp.arange(low, high)[None, :]
        slots = slots.reshape(-1)
        chosen = jnp.zeros((slots.shape[0], row_count), jnp.bool_)
        weighted = jnp.zeros((slots.shape[0], row_count), jnp.float32)
        for k in range(top_count):
            match = slots[:, None] == own_slots[:, k][None, :]
            chosen = chosen | match
            weighted = jnp.where(match, routed_expert_weight[:, k][None, :], weighted)
        picked = jnp.dot(
            chosen.astype(jnp.bfloat16), normed, preferred_element_type=jnp.float32
        ).astype(jnp.bfloat16)
        sent = picked.reshape(experts, (high - low) * sub, lane)
        arrived.append((weighted, sent_round(sent, SP)))
    answers = []
    for weighted, got in arrived:
        rows = got.reshape(-1, model_width)
        half = rows.shape[0] // 2
        blocks = ring_gathered(rows[:half], rows[half:], "tp")
        terms = expert_rows(
            blocks, expert_gate_weight[0], expert_up_weight[0], expert_down_weight[0]
        )
        first, second = ring_summed(terms, "tp")
        summed = jnp.concatenate([first, second], axis=0).astype(jnp.bfloat16)
        returned = sent_round(summed.reshape(got.shape), SP).reshape(-1, model_width)
        answers.append((weighted, returned))
    for weighted, returned in answers:
        routed_sum = routed_sum + lax.dot_general(
            weighted,
            returned.astype(jnp.float32),
            (((0,), (0,)), ((), ())),
            precision=lax.Precision.HIGHEST,
            preferred_element_type=jnp.float32,
        )
    return (mixed_wide + routed_sum).astype(jnp.bfloat16)


def solution(mesh):
    finer = Mesh(mesh.devices.reshape(8, 4, 2, mesh.shape["tp"]), ("sp_0", "sp_1", "sp_2", "tp"))
    placed = (
        P(SP, "tp"),
        P(SP, "tp"),
        P(SP, "tp"),
        P("tp", SP),
        P("tp", SP),
        P("tp", SP),
        P(SP_TP, None),
        P("tp", SP),
        P(),
        P(SP, None, "tp"),
        P(SP, None, "tp"),
        P(SP, "tp", None),
        P(SP, None),
        P(SP_TP, None),
    )
    return jax.shard_map(
        local, mesh=finer, in_specs=placed, out_specs=P(SP_TP, None), check_vma=False
    )
```

```python
import jax
import jax.numpy as jnp
from jax import lax
from jax.experimental import pallas as pl
from jax.experimental.pallas import tpu as pltpu
from jax.sharding import Mesh
from jax.sharding import PartitionSpec as P

SP = ("sp_0", "sp_1", "sp_2")
SP_TP = ("sp_0", "sp_1", "sp_2", "tp")


lowest = -1e30
epsilon = 1e-06


def sent_round(x, axis):
    return lax.all_to_all(x, axis, split_axis=0, concat_axis=0, tiled=True)


def shifted(x, axis, by):
    size = lax.axis_size(axis)
    return lax.ppermute(x, axis, [(i, (i + by) % size) for i in range(size)])


def terms_of(x, count):
    terms = []
    for _ in range(count):
        top = lax.reduce_precision(x, 8, 7)
        terms.append(top.astype(jnp.bfloat16))
        x = x - top
    return terms


def term_sum(x, count):
    parts = jnp.split(x.astype(jnp.float32), count, axis=-1)
    return sum(parts[1:], parts[0])


def side_row(parts, width):
    row = jnp.concatenate([term for part in parts for term in terms_of(part, 3)], axis=1)
    return jnp.pad(row, ((0, 0), (0, width - row.shape[1])))[:, None, :]


def earlier_state(final_log, mat, norm, peak, weight):
    size, heads = lax.axis_size(SP), final_log.shape[0]
    width = mat.shape[-1]
    per_slice = norm.size // size
    spots = jnp.arange(size)
    both = jnp.stack([final_log, peak], axis=1).reshape(1, -1)
    side = side_row(
        [norm.reshape(size, per_slice), jnp.broadcast_to(both, (size, both.shape[1]))], width
    )
    body = mat.reshape(size, -1, width)
    rows = body.shape[1]
    flat = weight.T
    columns = flat.shape[0]
    halves = jnp.stack([flat[:, :width], flat[:, width:]])
    for_all = jnp.broadcast_to(halves, (size // 2, *halves.shape)).reshape(size, columns, width)
    sent = jnp.concatenate([for_all, *terms_of(body, 2), side], axis=1)
    sent = jnp.pad(sent, ((0, 0), (0, -sent.shape[1] % 16), (0, 0)))
    got = sent_round(sent, SP)
    weight_rows = got[:, :columns].reshape(-1, width)
    got_mat = wide(got[:, columns : columns + rows]) + wide(
        got[:, columns + rows : columns + 2 * rows]
    )
    got_side = got[:, columns + 2 * rows]
    got_norm = term_sum(got_side[:, : 3 * per_slice], 3)
    scalars = term_sum(got_side[:, 3 * per_slice : 3 * per_slice + 6 * heads], 3)
    head = lax.axis_index(SP) * heads // size
    lane = jnp.arange(2 * heads)[None, :]
    logs = jnp.sum(jnp.where(lane == 2 * head, scalars, 0.0), axis=1)
    peaks = jnp.sum(jnp.where(lane == 2 * head + 1, scalars, 0.0), axis=1)
    between = (spots[None, None, :] < spots[:, None, None]) & (
        spots[None, None, :] > spots[None, :, None]
    )
    decay = jnp.sum(jnp.where(between, logs[None, None, :], 0.0), axis=-1)
    before = spots[None, :] < spots[:, None]
    level = jnp.where(before, peaks[None, :] + decay, lowest)
    top = jnp.max(level, axis=1)
    scale = jnp.where(before, jnp.exp(level - top[:, None]), 0.0)
    highest = lax.Precision.HIGHEST
    joined_mat = jnp.dot(scale, got_mat.reshape(size, -1), precision=highest)
    joined_norm = jnp.dot(scale, got_norm, precision=highest)
    back = jnp.concatenate(
        [
            joined_mat.reshape(size, rows, width).astype(jnp.bfloat16),
            side_row([joined_norm, top[:, None]], width),
        ],
        axis=1,
    )
    back = jnp.pad(back, ((0, 0), (0, -back.shape[1] % 8), (0, 0)))
    back = sent_round(back, SP)
    prior_mat = back[:, :rows].reshape(mat.shape)
    prior_norm = term_sum(back[:, rows, : 3 * per_slice], 3).reshape(norm.shape)
    prior_peak = term_sum(
        back[:: size // heads, rows, 3 * per_slice : 3 * per_slice + 3], 3
    )[:, 0]
    return prior_mat, prior_norm, prior_peak, weight_rows


def ring_gathered(first, second, axis):
    left_1 = shifted(first, axis, 1)
    right_2 = shifted(second, axis, -1)
    left_2 = shifted(second, axis, 1)
    right_1 = shifted(first, axis, -1)
    far_1 = shifted(left_1, axis, 1)
    far_2 = shifted(right_2, axis, -1)
    return (first, second, left_1, left_2, right_1, right_2, far_1, far_2)


def wide(x):
    return x.astype(jnp.float32)


def ring_summed(blocks, axis):
    own_1, own_2, left_1, left_2, right_1, right_2, far_1, far_2 = blocks
    far_in_1 = shifted(far_1, axis, 1)
    far_in_2 = shifted(far_2, axis, -1)
    from_left_2 = shifted(right_2, axis, 1)
    from_right_1 = shifted(left_1, axis, -1)
    from_left_1 = shifted((wide(right_1) + wide(far_in_1)).astype(jnp.bfloat16), axis, 1)
    from_right_2 = shifted((wide(left_2) + wide(far_in_2)).astype(jnp.bfloat16), axis, -1)
    first = wide(own_1) + wide(from_left_1) + wide(from_right_1)
    second = wide(own_2) + wide(from_left_2) + wide(from_right_2)
    return first, second


def expert_kernel(count, rows, tile, *refs):
    given, (gate, up, down) = refs[:count], refs[count : count + 3]
    outs = refs[count + 3 : 2 * count + 3]
    rows_in, rows_out, in_sems, out_sems = refs[2 * count + 3 :]
    entries = [
        pltpu.make_async_copy(given[k], rows_in.at[pl.ds(k * rows, rows)], in_sems.at[k])
        for k in range(count)
    ]
    for entry in entries:
        entry.start()
    for entry in entries:
        entry.wait()

    def one_tile(k, carry):
        here = pl.ds(pl.multiple_of(k * tile, tile), tile)
        x = rows_in[here, :]
        gate_pre = jnp.dot(x, gate[...], preferred_element_type=jnp.float32)
        up_pre = jnp.dot(x, up[...], preferred_element_type=jnp.float32)
        inner = (gate_pre / (1.0 + jnp.exp(-gate_pre)) * up_pre).astype(jnp.bfloat16)
        rows_out[here, :] = jnp.dot(
            inner, down[...], preferred_element_type=jnp.float32
        ).astype(jnp.bfloat16)
        return carry

    lax.fori_loop(0, count * rows // tile, one_tile, 0)
    stores = [
        pltpu.make_async_copy(rows_out.at[pl.ds(k * rows, rows)], outs[k], out_sems.at[k])
        for k in range(count)
    ]
    for store in stores:
        store.start()
    for store in stores:
        store.wait()


def expert_rows(blocks, gate_weight, up_weight, down_weight):
    count = len(blocks)
    rows, width = blocks[0].shape
    hidden = gate_weight.shape[1]
    anywhere = pl.BlockSpec(memory_space=pl.ANY)
    here = pl.BlockSpec(memory_space=pltpu.VMEM)
    return pl.pallas_call(
        lambda *refs: expert_kernel(count, rows, 256, *refs),
        out_shape=[jax.ShapeDtypeStruct((rows, width), jnp.bfloat16)] * count,
        in_specs=[anywhere] * count + [here] * 3,
        out_specs=[anywhere] * count,
        scratch_shapes=[
            pltpu.VMEM((count * rows, width), jnp.bfloat16),
            pltpu.VMEM((count * rows, width), jnp.bfloat16),
            pltpu.SemaphoreType.DMA((count,)),
            pltpu.SemaphoreType.DMA((count,)),
        ],
        compiler_params=pltpu.CompilerParams(vmem_limit_bytes=28 * 1024 * 1024),
        cost_estimate=pl.CostEstimate(
            flops=6 * count * rows * width * hidden,
            transcendentals=count * rows * hidden,
            bytes_accessed=6 * width * hidden + 4 * count * rows * width,
        ),
    )(*blocks, gate_weight, up_weight, down_weight)


def column(row, lanes=128):
    return jnp.transpose(jnp.broadcast_to(row, (lanes, row.shape[1])))


def summary_kernel(
    keys, values, gate_in, forget, extra, running_out, mat_out, norm_out, log_out, peak_out
):
    heads, length = gate_in.shape
    width = keys.shape[1] // heads
    raw = forget[...]
    running = jnp.minimum(raw, 0.0) - jnp.log1p(jnp.exp(-jnp.abs(raw))) + extra[...]
    lane = lax.broadcasted_iota(jnp.int32, running.shape, 1)
    step = 1
    while step < length:
        running = running + jnp.where(lane >= step, pltpu.roll(running, step, 1), 0.0)
        step *= 2
    running_out[...] = running
    final = running[:, length - 1 :]
    keep = final - running + gate_in[...]
    peak = jnp.max(keep, axis=1, keepdims=True)
    retain = jnp.exp(keep - peak)
    log_out[...] = jnp.broadcast_to(final, log_out.shape)
    peak_out[...] = jnp.broadcast_to(peak, peak_out.shape)
    for h in range(heads):
        mine = pl.ds(h * width, width)
        key = keys[:, mine]
        row = retain[h : h + 1]
        scaled = (column(row) * values[:, mine].astype(jnp.float32)).astype(jnp.bfloat16)
        mat_out[mine, :] = lax.dot_general(
            scaled, key, (((0,), (0,)), ((), ())), preferred_element_type=jnp.float32
        )
        norm_out[pl.ds(h, 1), :] = jnp.sum(
            column(row) * key.astype(jnp.float32), axis=0, keepdims=True
        )


def within_kernel(queries, keys, values, gate_in, running, numer_out, stats_out):
    heads, length = gate_in.shape
    width = keys.shape[1] // heads
    scale = width ** (-0.5)
    times = lax.broadcasted_iota(jnp.int32, (length, length), 0)
    sources = lax.broadcasted_iota(jnp.int32, (length, length), 1)
    causal = times >= sources
    place = lax.broadcasted_iota(jnp.int32, stats_out.shape, 1)
    stats = jnp.zeros(stats_out.shape, jnp.float32)
    for h in range(heads):
        mine = pl.ds(h * width, width)
        row = running[h : h + 1, :]
        down = column(row)[:, :1]
        level = jnp.where(causal, down - row + gate_in[h : h + 1, :], -jnp.inf)
        top = jnp.max(level, axis=1, keepdims=True)
        match = lax.dot_general(
            queries[:, mine],
            keys[:, mine],
            (((1,), (1,)), ((), ())),
            preferred_element_type=jnp.float32,
        )
        share = jnp.exp(level - top) * (match * scale)
        numer_out[:, mine] = jnp.dot(
            share.astype(jnp.bfloat16), values[:, mine], preferred_element_type=jnp.float32
        )
        total = jnp.sum(share, axis=1, keepdims=True)
        stats = jnp.where(place == 2 * h, total, stats)
        stats = jnp.where(place == 2 * h + 1, top, stats)
    stats_out[...] = stats


def finish_kernel(queries, running, numer, stats, mat, norm, peak, hidden_out):
    heads = running.shape[0]
    width = queries.shape[1] // heads
    scale = width ** (-0.5)
    for h in range(heads):
        mine = pl.ds(h * width, width)
        reached = column(running[h : h + 1, :])[:, :1] + peak[h : h + 1, :1]
        total = stats[:, 2 * h : 2 * h + 1]
        top = stats[:, 2 * h + 1 : 2 * h + 2]
        joined = jnp.maximum(top, reached)
        near = jnp.exp(top - joined)
        far = jnp.exp(reached - joined)
        query = queries[:, mine]
        past = lax.dot_general(
            query,
            mat[mine, :],
            (((1,), (1,)), ((), ())),
            preferred_element_type=jnp.float32,
        )
        past_total = jnp.sum(
            query.astype(jnp.float32) * norm[h : h + 1, :], axis=1, keepdims=True
        )
        upper = near * numer[:, mine] + far * (past * scale)
        lower = near * total + far * (past_total * scale)
        guarded = jnp.maximum(jnp.abs(lower), jnp.exp(-joined))
        hidden_out[:, mine] = (upper / guarded).astype(jnp.bfloat16)


def in_vmem(kernel, outs, *args):
    here = pl.BlockSpec(memory_space=pltpu.VMEM)
    return pl.pallas_call(
        kernel,
        out_shape=[jax.ShapeDtypeStruct(*out) for out in outs],
        in_specs=[here] * len(args),
        out_specs=[here] * len(outs),
        compiler_params=pltpu.CompilerParams(vmem_limit_bytes=12 * 1024 * 1024),
    )(*args)


def project_kernel(*refs):
    pieces, weights, others = refs[0], refs[1:6], refs[6:11]
    places, residual, gain, mixed_out, normed_out = refs[11:]
    half = weights[0].shape[1]
    is_first = places[0] == 0
    count = pieces.shape[0]
    shares = []
    for offset, blocks in ((0, (0,)), (count - 1, (1,)), (1, (2,)), (2, (3, 4))):
        piece = pieces[(places[1] + offset) % count]
        low, high = piece[:, :half], piece[:, half:]
        own = jnp.where(is_first, low, high)
        away = jnp.where(is_first, high, low)
        share = [
            lax.dot_general(
                own,
                weights[k][...],
                (((1,), (1,)), ((), ())),
                preferred_element_type=jnp.float32,
            )
            + lax.dot_general(
                away,
                others[k][...],
                (((1,), (1,)), ((), ())),
                preferred_element_type=jnp.float32,
            )
            for k in blocks
        ]
        share = jnp.concatenate(share, axis=1) if len(blocks) > 1 else share[0]
        shares.append(share.astype(jnp.bfloat16).astype(jnp.float32))
    projected = sum(shares[1:], shares[0])
    mixed = (residual[...].astype(jnp.float32) + projected).astype(jnp.bfloat16)
    mixed_out[...] = mixed
    mixed = mixed.astype(jnp.float32)
    norm_scale = lax.rsqrt(jnp.mean(mixed * mixed, axis=-1, keepdims=True) + epsilon)
    normed_out[...] = (mixed * norm_scale * gain[...]).astype(jnp.bfloat16)


def projection_weights(own):
    rows = own.shape[0] // 2
    left = shifted(own, "tp", 1)
    right = shifted(own, "tp", -1)
    far_1 = shifted(left[:rows], "tp", 1)
    far_2 = shifted(right[rows:], "tp", -1)
    weights = (own, left, right, far_1, far_2)
    return weights, tuple(shifted(piece, "sp_2", 1) for piece in weights)


def slot_index(ids, experts, capacity):
    flat_ids = ids.reshape(-1)
    matches = (flat_ids[:, None] == jnp.arange(experts, dtype=jnp.int32)[None, :]).astype(jnp.int32)
    before = jnp.cumsum(matches, axis=0) - matches
    return flat_ids * capacity + jnp.sum(before * matches, axis=1)


def local(
    memory_queries,
    memory_keys,
    memory_values,
    input_gate_logits,
    forget_gate_logits,
    extra_log_decay,
    residual,
    cell_output_weight,
    expert_norm_gain,
    expert_gate_weight,
    expert_up_weight,
    expert_down_weight,
    routed_expert_index,
    routed_expert_weight,
):
    f32, bf16 = jnp.float32, jnp.bfloat16
    heads, tokens = input_gate_logits.shape
    channels = memory_keys.shape[1]
    width = channels // heads
    running, mat, norm, final_log, peak = in_vmem(
        summary_kernel,
        (
            ((heads, tokens), f32),
            ((channels, width), f32),
            ((heads, width), f32),
            ((heads, width), f32),
            ((heads, width), f32),
        ),
        memory_keys,
        memory_values,
        input_gate_logits,
        forget_gate_logits,
        extra_log_decay,
    )
    prior_mat, prior_norm, prior_peak, own_rows = earlier_state(
        final_log[:, 0], mat, norm, peak[:, 0], cell_output_weight
    )
    weights, other_weights = projection_weights(own_rows)
    numer, stats = in_vmem(
        within_kernel,
        (((tokens, channels), f32), ((tokens, 128), f32)),
        memory_queries,
        memory_keys,
        memory_values,
        input_gate_logits,
        running,
    )
    (hidden,) = in_vmem(
        finish_kernel,
        (((tokens, channels), bf16),),
        memory_queries,
        running,
        numer,
        stats,
        prior_mat,
        prior_norm,
        jnp.broadcast_to(prior_peak[:, None], (heads, width)),
    )
    row_count, model_width = residual.shape
    place = lax.axis_index("tp")
    pieces = sent_round(hidden.reshape(-1, row_count, channels), "tp")
    here = pl.BlockSpec(memory_space=pltpu.VMEM)
    mixed_rows, normed = pl.pallas_call(
        project_kernel,
        out_shape=[jax.ShapeDtypeStruct(residual.shape, bf16)] * 2,
        in_specs=[here] * 11 + [pl.BlockSpec(memory_space=pltpu.SMEM)] + [here] * 2,
        out_specs=[here] * 2,
        compiler_params=pltpu.CompilerParams(vmem_limit_bytes=12 * 1024 * 1024),
        name="project_kernel",
    )(
        pieces,
        *weights,
        *other_weights,
        jnp.stack([lax.axis_index("sp_2"), place]),
        residual,
        expert_norm_gain[None, :],
    )
    mixed_wide = mixed_rows.astype(f32)
    sp_size = lax.axis_size(SP)
    top_count = routed_expert_index.shape[1]
    experts = sp_size * expert_gate_weight.shape[0]
    assigned = row_count * top_count
    capacity = max(2, assigned * 5 // (4 * experts))
    own_ids = lax.dynamic_slice_in_dim(routed_expert_index, place * row_count, row_count, 0)
    own_slots = slot_index(own_ids, experts, capacity).reshape(row_count, top_count)
    routed_sum = jnp.zeros((row_count, model_width), jnp.float32)
    chunks = ((0, 2), (2, 5))
    lane = 128
    sub = model_width // lane
    arrived = []
    for low, high in chunks:
        slots = jnp.arange(experts)[:, None] * capacity + jnp.arange(low, high)[None, :]
        slots = slots.reshape(-1)
        chosen = jnp.zeros((slots.shape[0], row_count), jnp.bool_)
        weighted = jnp.zeros((slots.shape[0], row_count), jnp.float32)
        for k in range(top_count):
            match = slots[:, None] == own_slots[:, k][None, :]
            chosen = chosen | match
            weighted = jnp.where(match, routed_expert_weight[:, k][None, :], weighted)
        picked = jnp.dot(
            chosen.astype(jnp.bfloat16), normed, preferred_element_type=jnp.float32
        ).astype(jnp.bfloat16)
        sent = picked.reshape(experts, (high - low) * sub, lane)
        arrived.append((weighted, sent_round(sent, SP)))
    answers = []
    for weighted, got in arrived:
        rows = got.reshape(-1, model_width)
        half = rows.shape[0] // 2
        blocks = ring_gathered(rows[:half], rows[half:], "tp")
        terms = expert_rows(
            blocks, expert_gate_weight[0], expert_up_weight[0], expert_down_weight[0]
        )
        first, second = ring_summed(terms, "tp")
        summed = jnp.concatenate([first, second], axis=0).astype(jnp.bfloat16)
        returned = sent_round(summed.reshape(got.shape), SP).reshape(-1, model_width)
        answers.append((weighted, returned))
    for weighted, returned in answers:
        routed_sum = routed_sum + lax.dot_general(
            weighted,
            returned.astype(jnp.float32),
            (((0,), (0,)), ((), ())),
            precision=lax.Precision.HIGHEST,
            preferred_element_type=jnp.float32,
        )
    return (mixed_wide + routed_sum).astype(jnp.bfloat16)


def solution(mesh):
    finer = Mesh(mesh.devices.reshape(8, 4, 2, mesh.shape["tp"]), ("sp_0", "sp_1", "sp_2", "tp"))
    placed = (
        P(SP, "tp"),
        P(SP, "tp"),
        P(SP, "tp"),
        P("tp", SP),
        P("tp", SP),
        P("tp", SP),
        P(SP_TP, None),
        P("tp", SP),
        P(),
        P(SP, None, "tp"),
        P(SP, None, "tp"),
        P(SP, "tp", None),
        P(SP, None),
        P(SP_TP, None),
    )
    return jax.shard_map(
        local, mesh=finer, in_specs=placed, out_specs=P(SP_TP, None), check_vma=False
    )
```

```python
import jax
import jax.numpy as jnp
from jax import lax
from jax.experimental import pallas as pl
from jax.experimental.pallas import tpu as pltpu
from jax.sharding import Mesh
from jax.sharding import PartitionSpec as P

SP = ("sp_0", "sp_1", "sp_2")
SP_TP = ("sp_0", "sp_1", "sp_2", "tp")


lowest = -1e30
epsilon = 1e-06


def sent_round(x, axis):
    return lax.all_to_all(x, axis, split_axis=0, concat_axis=0, tiled=True)


def shifted(x, axis, by):
    size = lax.axis_size(axis)
    return lax.ppermute(x, axis, [(i, (i + by) % size) for i in range(size)])


def terms_of(x, count):
    terms = []
    for _ in range(count):
        top = lax.reduce_precision(x, 8, 7)
        terms.append(top.astype(jnp.bfloat16))
        x = x - top
    return terms


def term_sum(x, count):
    parts = jnp.split(x.astype(jnp.float32), count, axis=-1)
    return sum(parts[1:], parts[0])


def side_row(parts, width):
    row = jnp.concatenate([term for part in parts for term in terms_of(part, 3)], axis=1)
    return jnp.pad(row, ((0, 0), (0, width - row.shape[1])))[:, None, :]


def earlier_state(final_log, mat, norm, peak, weight):
    size, heads = lax.axis_size(SP), final_log.shape[0]
    width = mat.shape[-1]
    per_slice = norm.size // size
    spots = jnp.arange(size)
    both = jnp.stack([final_log, peak], axis=1).reshape(1, -1)
    side = side_row(
        [norm.reshape(size, per_slice), jnp.broadcast_to(both, (size, both.shape[1]))], width
    )
    body = mat.reshape(size, -1, width)
    rows = body.shape[1]
    flat = weight.T
    columns = flat.shape[0]
    halves = jnp.stack([flat[:, :width], flat[:, width:]])
    for_all = jnp.broadcast_to(halves, (size // 2, *halves.shape)).reshape(size, columns, width)
    sent = jnp.concatenate([for_all, *terms_of(body, 2), side], axis=1)
    sent = jnp.pad(sent, ((0, 0), (0, -sent.shape[1] % 16), (0, 0)))
    got = sent_round(sent, SP)
    weight_rows = got[:, :columns].reshape(-1, width)
    got_mat = wide(got[:, columns : columns + rows]) + wide(
        got[:, columns + rows : columns + 2 * rows]
    )
    got_side = got[:, columns + 2 * rows]
    got_norm = term_sum(got_side[:, : 3 * per_slice], 3)
    scalars = term_sum(got_side[:, 3 * per_slice : 3 * per_slice + 6 * heads], 3)
    head = lax.axis_index(SP) * heads // size
    lane = jnp.arange(2 * heads)[None, :]
    logs = jnp.sum(jnp.where(lane == 2 * head, scalars, 0.0), axis=1)
    peaks = jnp.sum(jnp.where(lane == 2 * head + 1, scalars, 0.0), axis=1)
    between = (spots[None, None, :] < spots[:, None, None]) & (
        spots[None, None, :] > spots[None, :, None]
    )
    decay = jnp.sum(jnp.where(between, logs[None, None, :], 0.0), axis=-1)
    before = spots[None, :] < spots[:, None]
    level = jnp.where(before, peaks[None, :] + decay, lowest)
    top = jnp.max(level, axis=1)
    scale = jnp.where(before, jnp.exp(level - top[:, None]), 0.0)
    highest = lax.Precision.HIGHEST
    joined_mat = jnp.dot(scale, got_mat.reshape(size, -1), precision=highest)
    joined_norm = jnp.dot(scale, got_norm, precision=highest)
    back = jnp.concatenate(
        [
            joined_mat.reshape(size, rows, width).astype(jnp.bfloat16),
            side_row([joined_norm, top[:, None]], width),
        ],
        axis=1,
    )
    back = jnp.pad(back, ((0, 0), (0, -back.shape[1] % 8), (0, 0)))
    back = sent_round(back, SP)
    prior_mat = back[:, :rows].reshape(mat.shape)
    side = lax.optimization_barrier(back[:, rows])
    prior_norm = term_sum(side[:, : 3 * per_slice], 3).reshape(norm.shape)
    prior_peak = term_sum(side[:: size // heads, 3 * per_slice : 3 * per_slice + 3], 3)[:, 0]
    return prior_mat, prior_norm, prior_peak, weight_rows


def ring_gathered(first, second, axis):
    left_1 = shifted(first, axis, 1)
    right_2 = shifted(second, axis, -1)
    left_2 = shifted(second, axis, 1)
    right_1 = shifted(first, axis, -1)
    far_1 = shifted(left_1, axis, 1)
    far_2 = shifted(right_2, axis, -1)
    return (first, second, left_1, left_2, right_1, right_2, far_1, far_2)


def wide(x):
    return x.astype(jnp.float32)


def ring_summed(blocks, axis):
    own_1, own_2, left_1, left_2, right_1, right_2, far_1, far_2 = blocks
    far_in_1 = shifted(far_1, axis, 1)
    far_in_2 = shifted(far_2, axis, -1)
    from_left_2 = shifted(right_2, axis, 1)
    from_right_1 = shifted(left_1, axis, -1)
    from_left_1 = shifted((wide(right_1) + wide(far_in_1)).astype(jnp.bfloat16), axis, 1)
    from_right_2 = shifted((wide(left_2) + wide(far_in_2)).astype(jnp.bfloat16), axis, -1)
    first = wide(own_1) + wide(from_left_1) + wide(from_right_1)
    second = wide(own_2) + wide(from_left_2) + wide(from_right_2)
    return first, second


def expert_kernel(count, rows, tile, *refs):
    given, sources = refs[:count], refs[count : count + 3]
    outs = refs[count + 3 : 2 * count + 3]
    rows_in, rows_out, gate, up, down, in_sems, out_sems, weight_sems = refs[2 * count + 3 :]
    copies = [
        pltpu.make_async_copy(source, weight, weight_sems.at[k])
        for k, (source, weight) in enumerate(zip(sources, (gate, up, down)))
    ]
    entries = [
        pltpu.make_async_copy(given[k], rows_in.at[pl.ds(k * rows, rows)], in_sems.at[k])
        for k in range(count)
    ]
    for copy in copies[:1] + entries + copies[1:]:
        copy.start()
    for entry in entries:
        entry.wait()

    def one_tile(k, carry):
        here = pl.ds(pl.multiple_of(k * tile, tile), tile)
        x = rows_in[here, :]
        pl.when(k == 0)(copies[0].wait)
        gate_pre = jnp.dot(x, gate[...], preferred_element_type=jnp.float32)
        pl.when(k == 0)(copies[1].wait)
        up_pre = jnp.dot(x, up[...], preferred_element_type=jnp.float32)
        inner = (gate_pre / (1.0 + jnp.exp(-gate_pre)) * up_pre).astype(jnp.bfloat16)
        pl.when(k == 0)(copies[2].wait)
        rows_out[here, :] = jnp.dot(
            inner, down[...], preferred_element_type=jnp.float32
        ).astype(jnp.bfloat16)
        return carry

    lax.fori_loop(0, count * rows // tile, one_tile, 0)
    stores = [
        pltpu.make_async_copy(rows_out.at[pl.ds(k * rows, rows)], outs[k], out_sems.at[k])
        for k in range(count)
    ]
    for store in stores:
        store.start()
    for store in stores:
        store.wait()


def expert_rows(blocks, weights):
    count = len(blocks)
    rows, width = blocks[0].shape
    hidden = weights[0].shape[1]
    anywhere = pl.BlockSpec(memory_space=pl.ANY)
    return pl.pallas_call(
        lambda *refs: expert_kernel(count, rows, 256, *refs),
        out_shape=[jax.ShapeDtypeStruct((rows, width), jnp.bfloat16)] * count,
        in_specs=[anywhere] * (count + 3),
        out_specs=[anywhere] * count,
        scratch_shapes=[
            pltpu.VMEM((count * rows, width), jnp.bfloat16),
            pltpu.VMEM((count * rows, width), jnp.bfloat16),
            *(pltpu.VMEM(w.shape, w.dtype) for w in weights),
            pltpu.SemaphoreType.DMA((count,)),
            pltpu.SemaphoreType.DMA((count,)),
            pltpu.SemaphoreType.DMA((3,)),
        ],
        compiler_params=pltpu.CompilerParams(vmem_limit_bytes=46 * 1024 * 1024),
        cost_estimate=pl.CostEstimate(
            flops=6 * count * rows * width * hidden,
            transcendentals=count * rows * hidden,
            bytes_accessed=6 * width * hidden + 4 * count * rows * width,
        ),
    )(*blocks, *weights)


def column(row, lanes=128):
    return jnp.transpose(jnp.broadcast_to(row, (lanes, row.shape[1])))


def summary_kernel(
    keys, values, gate_in, forget, extra, running_out, mat_out, norm_out, log_out, peak_out
):
    heads, length = gate_in.shape
    width = keys.shape[1] // heads
    raw = forget[...]
    running = jnp.minimum(raw, 0.0) - jnp.log1p(jnp.exp(-jnp.abs(raw))) + extra[...]
    lane = lax.broadcasted_iota(jnp.int32, running.shape, 1)
    step = 1
    while step < length:
        running = running + jnp.where(lane >= step, pltpu.roll(running, step, 1), 0.0)
        step *= 2
    running_out[...] = running
    final = running[:, length - 1 :]
    keep = final - running + gate_in[...]
    peak = jnp.max(keep, axis=1, keepdims=True)
    retain = jnp.exp(keep - peak)
    log_out[...] = jnp.broadcast_to(final, log_out.shape)
    peak_out[...] = jnp.broadcast_to(peak, peak_out.shape)
    for h in range(heads):
        mine = pl.ds(h * width, width)
        key = keys[:, mine]
        row = retain[h : h + 1]
        scaled = (column(row) * values[:, mine].astype(jnp.float32)).astype(jnp.bfloat16)
        mat_out[mine, :] = lax.dot_general(
            scaled, key, (((0,), (0,)), ((), ())), preferred_element_type=jnp.float32
        )
        norm_out[pl.ds(h, 1), :] = jnp.sum(
            column(row) * key.astype(jnp.float32), axis=0, keepdims=True
        )


def within_kernel(queries, keys, values, gate_in, running, numer_out, stats_out):
    heads, length = gate_in.shape
    width = keys.shape[1] // heads
    scale = width ** (-0.5)
    times = lax.broadcasted_iota(jnp.int32, (length, length), 0)
    sources = lax.broadcasted_iota(jnp.int32, (length, length), 1)
    causal = times >= sources
    place = lax.broadcasted_iota(jnp.int32, stats_out.shape, 1)
    stats = jnp.zeros(stats_out.shape, jnp.float32)
    for h in range(heads):
        mine = pl.ds(h * width, width)
        row = running[h : h + 1, :]
        down = column(row)[:, :1]
        level = jnp.where(causal, down - row + gate_in[h : h + 1, :], -jnp.inf)
        top = jnp.max(level, axis=1, keepdims=True)
        match = lax.dot_general(
            queries[:, mine],
            keys[:, mine],
            (((1,), (1,)), ((), ())),
            preferred_element_type=jnp.float32,
        )
        share = jnp.exp(level - top) * (match * scale)
        numer_out[:, mine] = jnp.dot(
            share.astype(jnp.bfloat16), values[:, mine], preferred_element_type=jnp.float32
        )
        total = jnp.sum(share, axis=1, keepdims=True)
        stats = jnp.where(place == 2 * h, total, stats)
        stats = jnp.where(place == 2 * h + 1, top, stats)
    stats_out[...] = stats


def finish_kernel(queries, running, numer, stats, mat, norm, peak, hidden_out):
    heads = running.shape[0]
    width = queries.shape[1] // heads
    scale = width ** (-0.5)
    for h in range(heads):
        mine = pl.ds(h * width, width)
        reached = column(running[h : h + 1, :])[:, :1] + peak[h : h + 1, :1]
        total = stats[:, 2 * h : 2 * h + 1]
        top = stats[:, 2 * h + 1 : 2 * h + 2]
        joined = jnp.maximum(top, reached)
        near = jnp.exp(top - joined)
        far = jnp.exp(reached - joined)
        query = queries[:, mine]
        past = lax.dot_general(
            query,
            mat[mine, :],
            (((1,), (1,)), ((), ())),
            preferred_element_type=jnp.float32,
        )
        past_total = jnp.sum(
            query.astype(jnp.float32) * norm[h : h + 1, :], axis=1, keepdims=True
        )
        upper = near * numer[:, mine] + far * (past * scale)
        lower = near * total + far * (past_total * scale)
        guarded = jnp.maximum(jnp.abs(lower), jnp.exp(-joined))
        hidden_out[:, mine] = (upper / guarded).astype(jnp.bfloat16)


def in_vmem(kernel, outs, *args, limit=12):
    return pl.pallas_call(
        kernel,
        out_shape=[jax.ShapeDtypeStruct(*out) for out in outs],
        compiler_params=pltpu.CompilerParams(vmem_limit_bytes=limit * 1024 * 1024),
    )(*args)


def project_kernel(*refs):
    pieces, weights, others = refs[0], refs[1:5], refs[5:9]
    places, residual, gain, mixed_out, normed_out = refs[9:]
    half = weights[0].shape[1]
    is_first = places[0] == 0
    count = pieces.shape[0]
    shares = []
    for k, offset in enumerate((0, count - 1, 1, 2)):
        piece = pieces[(places[1] + offset) % count]
        low, high = piece[:, :half], piece[:, half:]
        own = jnp.where(is_first, low, high)
        away = jnp.where(is_first, high, low)
        share = lax.dot_general(
            own,
            weights[k][...],
            (((1,), (1,)), ((), ())),
            preferred_element_type=jnp.float32,
        ) + lax.dot_general(
            away,
            others[k][...],
            (((1,), (1,)), ((), ())),
            preferred_element_type=jnp.float32,
        )
        shares.append(share.astype(jnp.bfloat16).astype(jnp.float32))
    projected = sum(shares[1:], shares[0])
    mixed = (residual[...].astype(jnp.float32) + projected).astype(jnp.bfloat16)
    mixed_out[...] = mixed
    mixed = mixed.astype(jnp.float32)
    norm_scale = lax.rsqrt(jnp.mean(mixed * mixed, axis=-1, keepdims=True) + epsilon)
    normed_out[...] = (mixed * norm_scale * gain[...]).astype(jnp.bfloat16)


def projection_weights(own):
    weights = (own, *(shifted(own, "tp", by) for by in (1, -1, 2)))
    others = []
    for piece in weights:
        others.append(shifted(piece, "sp_2", 1))
    return weights, others


def slot_index(ids, experts, capacity):
    flat_ids = ids.reshape(-1)
    matches = (flat_ids[:, None] == jnp.arange(experts, dtype=jnp.int32)[None, :]).astype(jnp.int32)
    before = jnp.cumsum(matches, axis=0) - matches
    return flat_ids * capacity + jnp.sum(before * matches, axis=1)


def slot_masks(own_slots, routed_weight, chunks, experts, capacity):
    masks = []
    for low, high in chunks:
        slots = jnp.arange(experts)[:, None] * capacity + jnp.arange(low, high)[None, :]
        slots = slots.reshape(-1)
        chosen = jnp.zeros((slots.shape[0], own_slots.shape[0]), jnp.bool_)
        weighted = jnp.zeros(chosen.shape, jnp.float32)
        for k in range(own_slots.shape[1]):
            match = slots[:, None] == own_slots[:, k][None, :]
            chosen = chosen | match
            weighted = jnp.where(match, routed_weight[:, k][None, :], weighted)
        masks.append(lax.optimization_barrier((chosen.astype(jnp.bfloat16), weighted)))
    return masks


def local(
    memory_queries,
    memory_keys,
    memory_values,
    input_gate_logits,
    forget_gate_logits,
    extra_log_decay,
    residual,
    cell_output_weight,
    expert_norm_gain,
    expert_gate_weight,
    expert_up_weight,
    expert_down_weight,
    routed_expert_index,
    routed_expert_weight,
):
    f32, bf16 = jnp.float32, jnp.bfloat16
    heads, tokens = input_gate_logits.shape
    channels = memory_keys.shape[1]
    width = channels // heads
    running, mat, norm, final_log, peak = in_vmem(
        summary_kernel,
        (
            ((heads, tokens), f32),
            ((channels, width), f32),
            ((heads, width), f32),
            ((heads, width), f32),
            ((heads, width), f32),
        ),
        memory_keys,
        memory_values,
        input_gate_logits,
        forget_gate_logits,
        extra_log_decay,
        limit=60,
    )
    prior_mat, prior_norm, prior_peak, own_rows = earlier_state(
        final_log[:, 0], mat, norm, peak[:, 0], cell_output_weight
    )
    weights, other_weights = projection_weights(own_rows)
    numer, stats = in_vmem(
        within_kernel,
        (((tokens, channels), f32), ((tokens, 128), f32)),
        memory_queries,
        memory_keys,
        memory_values,
        input_gate_logits,
        running,
    )
    (hidden,) = in_vmem(
        finish_kernel,
        (((tokens, channels), bf16),),
        memory_queries,
        running,
        numer,
        stats,
        prior_mat,
        prior_norm,
        jnp.broadcast_to(prior_peak[:, None], (heads, width)),
    )
    row_count, model_width = residual.shape
    place = lax.axis_index("tp")
    pieces = sent_round(hidden.reshape(-1, row_count, channels), "tp")
    here = pl.BlockSpec()
    mixed_rows, normed = pl.pallas_call(
        project_kernel,
        out_shape=[jax.ShapeDtypeStruct(residual.shape, bf16)] * 2,
        in_specs=[here] * 9 + [pl.BlockSpec(memory_space=pltpu.SMEM)] + [here] * 2,
        compiler_params=pltpu.CompilerParams(vmem_limit_bytes=12 * 1024 * 1024),
        name="project_kernel",
    )(
        pieces,
        *weights,
        *other_weights,
        jnp.stack([lax.axis_index("sp_2"), place]),
        residual,
        expert_norm_gain[None, :],
    )
    mixed_wide = mixed_rows.astype(f32)
    sp_size = lax.axis_size(SP)
    top_count = routed_expert_index.shape[1]
    experts = sp_size * expert_gate_weight.shape[0]
    assigned = row_count * top_count
    capacity = max(2, assigned * 5 // (4 * experts))
    own_ids = lax.dynamic_slice_in_dim(routed_expert_index, place * row_count, row_count, 0)
    chunks = ((0, 2), (2, 5))
    own_slots = slot_index(own_ids, experts, capacity).reshape(row_count, top_count)
    masks = slot_masks(own_slots, routed_expert_weight, chunks, experts, capacity)
    routed_sum = jnp.zeros((row_count, model_width), jnp.float32)
    lane = 128
    sub = model_width // lane
    arrived = []
    for (low, high), (chosen, weighted) in zip(chunks, masks):
        picked = jnp.dot(
            chosen, normed, preferred_element_type=jnp.float32
        ).astype(jnp.bfloat16)
        sent = picked.reshape(experts, (high - low) * sub, lane)
        arrived.append((weighted, sent_round(sent, SP)))
    weights_here = (expert_gate_weight[0], expert_up_weight[0], expert_down_weight[0])
    answers = []
    for weighted, got in arrived:
        rows = got.reshape(-1, model_width)
        half = rows.shape[0] // 2
        blocks = ring_gathered(rows[:half], rows[half:], "tp")
        terms = expert_rows(blocks, weights_here)
        first, second = ring_summed(terms, "tp")
        summed = jnp.concatenate([first, second], axis=0).astype(jnp.bfloat16)
        returned = sent_round(summed.reshape(got.shape), SP).reshape(-1, model_width)
        answers.append((weighted, returned))
    for weighted, returned in answers:
        routed_sum = routed_sum + lax.dot_general(
            weighted,
            returned.astype(jnp.float32),
            (((0,), (0,)), ((), ())),
            precision=lax.Precision.HIGHEST,
            preferred_element_type=jnp.float32,
        )
    return (mixed_wide + routed_sum).astype(jnp.bfloat16)


def solution(mesh):
    finer = Mesh(mesh.devices.reshape(8, 4, 2, mesh.shape["tp"]), ("sp_0", "sp_1", "sp_2", "tp"))
    placed = (
        P(SP, "tp"),
        P(SP, "tp"),
        P(SP, "tp"),
        P("tp", SP),
        P("tp", SP),
        P("tp", SP),
        P(SP_TP, None),
        P("tp", SP),
        P(),
        P(SP, None, "tp"),
        P(SP, None, "tp"),
        P(SP, "tp", None),
        P(SP, None),
        P(SP_TP, None),
    )
    return jax.shard_map(
        local, mesh=finer, in_specs=placed, out_specs=P(SP_TP, None), check_vma=False
    )
```

```python
import jax
import jax.numpy as jnp
from jax import lax
from jax.experimental import pallas as pl
from jax.experimental.pallas import tpu as pltpu
from jax.sharding import Mesh
from jax.sharding import PartitionSpec as P

SP = ("sp_0", "sp_1", "sp_2")
SP_TP = ("sp_0", "sp_1", "sp_2", "tp")


lowest = -1e30
epsilon = 1e-06


def sent_round(x, axis):
    return lax.all_to_all(x, axis, split_axis=0, concat_axis=0, tiled=True)


def shifted(x, axis, by):
    size = lax.axis_size(axis)
    return lax.ppermute(x, axis, [(i, (i + by) % size) for i in range(size)])


def terms_of(x, count):
    terms = []
    for _ in range(count):
        top = lax.reduce_precision(x, 8, 7)
        terms.append(top.astype(jnp.bfloat16))
        x = x - top
    return terms


def term_sum(x, count):
    parts = jnp.split(x.astype(jnp.float32), count, axis=-1)
    return sum(parts[1:], parts[0])


def side_row(parts, width):
    row = jnp.concatenate([term for part in parts for term in terms_of(part, 3)], axis=1)
    return jnp.pad(row, ((0, 0), (0, width - row.shape[1])))[:, None, :]


def earlier_state(final_log, mat, norm, peak, weight):
    size, heads = lax.axis_size(SP), final_log.shape[0]
    width = mat.shape[-1]
    per_slice = norm.size // size
    spots = jnp.arange(size)
    both = jnp.stack([final_log, peak], axis=1).reshape(1, -1)
    side = side_row(
        [norm.reshape(size, per_slice), jnp.broadcast_to(both, (size, both.shape[1]))], width
    )
    body = mat.reshape(size, -1, width)
    rows = body.shape[1]
    flat = weight.T
    columns = flat.shape[0]
    halves = jnp.stack([flat[:, :width], flat[:, width:]])
    for_all = jnp.broadcast_to(halves, (size // 2, *halves.shape)).reshape(size, columns, width)
    sent = jnp.concatenate([for_all, *terms_of(body, 2), side], axis=1)
    sent = jnp.pad(sent, ((0, 0), (0, -sent.shape[1] % 16), (0, 0)))
    got = sent_round(sent, SP)
    weight_rows = got[:, :columns].reshape(-1, width)
    got_mat = wide(got[:, columns : columns + rows]) + wide(
        got[:, columns + rows : columns + 2 * rows]
    )
    got_side = got[:, columns + 2 * rows]
    got_norm = term_sum(got_side[:, : 3 * per_slice], 3)
    scalars = term_sum(got_side[:, 3 * per_slice : 3 * per_slice + 6 * heads], 3)
    head = lax.axis_index(SP) * heads // size
    lane = jnp.arange(2 * heads)[None, :]
    logs = jnp.sum(jnp.where(lane == 2 * head, scalars, 0.0), axis=1)
    peaks = jnp.sum(jnp.where(lane == 2 * head + 1, scalars, 0.0), axis=1)
    between = (spots[None, None, :] < spots[:, None, None]) & (
        spots[None, None, :] > spots[None, :, None]
    )
    decay = jnp.sum(jnp.where(between, logs[None, None, :], 0.0), axis=-1)
    before = spots[None, :] < spots[:, None]
    level = jnp.where(before, peaks[None, :] + decay, lowest)
    top = jnp.max(level, axis=1)
    scale = jnp.where(before, jnp.exp(level - top[:, None]), 0.0)
    highest = lax.Precision.HIGHEST
    joined_mat = jnp.dot(scale, got_mat.reshape(size, -1), precision=highest)
    joined_norm = jnp.dot(scale, got_norm, precision=highest)
    back = jnp.concatenate(
        [
            joined_mat.reshape(size, rows, width).astype(jnp.bfloat16),
            side_row([joined_norm, top[:, None]], width),
        ],
        axis=1,
    )
    back = jnp.pad(back, ((0, 0), (0, -back.shape[1] % 8), (0, 0)))
    back = sent_round(back, SP)
    prior_mat = back[:, :rows].reshape(mat.shape)
    side = lax.optimization_barrier(back[:, rows])
    prior_norm = term_sum(side[:, : 3 * per_slice], 3).reshape(norm.shape)
    prior_peak = term_sum(side[:: size // heads, 3 * per_slice : 3 * per_slice + 3], 3)[:, 0]
    return prior_mat, prior_norm, prior_peak, weight_rows


def ring_gathered(first, second, axis):
    left_1 = shifted(first, axis, 1)
    right_2 = shifted(second, axis, -1)
    left_2 = shifted(second, axis, 1)
    right_1 = shifted(first, axis, -1)
    far_1 = shifted(left_1, axis, 1)
    far_2 = shifted(right_2, axis, -1)
    return (first, second, left_1, left_2, right_1, right_2, far_1, far_2)


def wide(x):
    return x.astype(jnp.float32)


def ring_summed(blocks, axis):
    own_1, own_2, left_1, left_2, right_1, right_2, far_1, far_2 = blocks
    far_in_1 = shifted(far_1, axis, 1)
    far_in_2 = shifted(far_2, axis, -1)
    from_left_2 = shifted(right_2, axis, 1)
    from_right_1 = shifted(left_1, axis, -1)
    from_left_1 = shifted((wide(right_1) + wide(far_in_1)).astype(jnp.bfloat16), axis, 1)
    from_right_2 = shifted((wide(left_2) + wide(far_in_2)).astype(jnp.bfloat16), axis, -1)
    first = wide(own_1) + wide(from_left_1) + wide(from_right_1)
    second = wide(own_2) + wide(from_left_2) + wide(from_right_2)
    return first, second


def expert_kernel(count, rows, per_tile, *refs):
    given, (gate, up, down) = refs[:count], refs[count : count + 3]
    outs = refs[count + 3 : 2 * count + 3]
    rows_in, rows_out, in_sems, out_sems = refs[2 * count + 3 :]
    entries = [
        pltpu.make_async_copy(given[k], rows_in.at[pl.ds(k * rows, rows)], in_sems.at[k])
        for k in range(count)
    ]
    stores = [
        pltpu.make_async_copy(rows_out.at[pl.ds(k * rows, rows)], outs[k], out_sems.at[k])
        for k in range(count)
    ]
    tile = per_tile * rows
    tiles = count // per_tile
    for entry in entries:
        entry.start()

    def at_tile(k, action, copies):
        for here in range(tiles):

            @pl.when(k == here)
            def _():
                for copy in copies[here * per_tile : (here + 1) * per_tile]:
                    getattr(copy, action)()

    def one_tile(k, carry):
        here = pl.ds(pl.multiple_of(k * tile, tile), tile)
        at_tile(k, "wait", entries)
        x = rows_in[here, :]
        gate_pre = jnp.dot(x, gate[...], preferred_element_type=jnp.float32)
        up_pre = jnp.dot(x, up[...], preferred_element_type=jnp.float32)
        inner = (gate_pre / (1.0 + jnp.exp(-gate_pre)) * up_pre).astype(jnp.bfloat16)
        rows_out[here, :] = jnp.dot(
            inner, down[...], preferred_element_type=jnp.float32
        ).astype(jnp.bfloat16)
        at_tile(k, "start", stores)
        return carry

    lax.fori_loop(0, tiles, one_tile, 0)
    for store in stores:
        store.wait()


def expert_rows(blocks, weights, per_tile):
    count = len(blocks)
    rows, width = blocks[0].shape
    hidden = weights[0].shape[1]
    anywhere = pl.BlockSpec(memory_space=pl.ANY)
    here = pl.BlockSpec(memory_space=pltpu.VMEM)
    return pl.pallas_call(
        lambda *refs: expert_kernel(count, rows, per_tile, *refs),
        out_shape=[jax.ShapeDtypeStruct((rows, width), jnp.bfloat16)] * count,
        in_specs=[anywhere] * count + [here] * 3,
        out_specs=[anywhere] * count,
        scratch_shapes=[
            pltpu.VMEM((count * rows, width), jnp.bfloat16),
            pltpu.VMEM((count * rows, width), jnp.bfloat16),
            pltpu.SemaphoreType.DMA((count,)),
            pltpu.SemaphoreType.DMA((count,)),
        ],
        compiler_params=pltpu.CompilerParams(vmem_limit_bytes=28 * 1024 * 1024),
        cost_estimate=pl.CostEstimate(
            flops=6 * count * rows * width * hidden,
            transcendentals=count * rows * hidden,
            bytes_accessed=6 * width * hidden + 4 * count * rows * width,
        ),
    )(*blocks, *weights)


def column(row, lanes=128):
    return jnp.transpose(jnp.broadcast_to(row, (lanes, row.shape[1])))


def summary_kernel(
    keys, values, gate_in, forget, extra, running_out, mat_out, norm_out, log_out, peak_out
):
    heads, length = gate_in.shape
    width = keys.shape[1] // heads
    raw = forget[...]
    running = jnp.minimum(raw, 0.0) - jnp.log1p(jnp.exp(-jnp.abs(raw))) + extra[...]
    lane = lax.broadcasted_iota(jnp.int32, running.shape, 1)
    step = 1
    while step < length:
        running = running + jnp.where(lane >= step, pltpu.roll(running, step, 1), 0.0)
        step *= 2
    running_out[...] = running
    final = running[:, length - 1 :]
    keep = final - running + gate_in[...]
    peak = jnp.max(keep, axis=1, keepdims=True)
    retain = jnp.exp(keep - peak)
    log_out[...] = jnp.broadcast_to(final, log_out.shape)
    peak_out[...] = jnp.broadcast_to(peak, peak_out.shape)
    for h in range(heads):
        mine = pl.ds(h * width, width)
        key = keys[:, mine]
        row = retain[h : h + 1]
        scaled = (column(row) * values[:, mine].astype(jnp.float32)).astype(jnp.bfloat16)
        mat_out[mine, :] = lax.dot_general(
            scaled, key, (((0,), (0,)), ((), ())), preferred_element_type=jnp.float32
        )
        norm_out[pl.ds(h, 1), :] = jnp.sum(
            column(row) * key.astype(jnp.float32), axis=0, keepdims=True
        )


def within_kernel(queries, keys, values, gate_in, running, numer_out, stats_out):
    heads, length = gate_in.shape
    width = keys.shape[1] // heads
    scale = width ** (-0.5)
    times = lax.broadcasted_iota(jnp.int32, (length, length), 0)
    sources = lax.broadcasted_iota(jnp.int32, (length, length), 1)
    causal = times >= sources
    place = lax.broadcasted_iota(jnp.int32, stats_out.shape, 1)
    stats = jnp.zeros(stats_out.shape, jnp.float32)
    for h in range(heads):
        mine = pl.ds(h * width, width)
        row = running[h : h + 1, :]
        down = column(row)[:, :1]
        level = jnp.where(causal, down - row + gate_in[h : h + 1, :], -jnp.inf)
        top = jnp.max(level, axis=1, keepdims=True)
        match = lax.dot_general(
            queries[:, mine],
            keys[:, mine],
            (((1,), (1,)), ((), ())),
            preferred_element_type=jnp.float32,
        )
        share = jnp.exp(level - top) * (match * scale)
        numer_out[:, mine] = jnp.dot(
            share.astype(jnp.bfloat16), values[:, mine], preferred_element_type=jnp.float32
        )
        total = jnp.sum(share, axis=1, keepdims=True)
        stats = jnp.where(place == 2 * h, total, stats)
        stats = jnp.where(place == 2 * h + 1, top, stats)
    stats_out[...] = stats


def finish_kernel(queries, running, numer, stats, mat, norm, peak, hidden_out):
    heads = running.shape[0]
    width = queries.shape[1] // heads
    scale = width ** (-0.5)
    for h in range(heads):
        mine = pl.ds(h * width, width)
        reached = column(running[h : h + 1, :])[:, :1] + peak[h : h + 1, :1]
        total = stats[:, 2 * h : 2 * h + 1]
        top = stats[:, 2 * h + 1 : 2 * h + 2]
        joined = jnp.maximum(top, reached)
        near = jnp.exp(top - joined)
        far = jnp.exp(reached - joined)
        query = queries[:, mine]
        past = lax.dot_general(
            query,
            mat[mine, :],
            (((1,), (1,)), ((), ())),
            preferred_element_type=jnp.float32,
        )
        past_total = jnp.sum(
            query.astype(jnp.float32) * norm[h : h + 1, :], axis=1, keepdims=True
        )
        upper = near * numer[:, mine] + far * (past * scale)
        lower = near * total + far * (past_total * scale)
        guarded = jnp.maximum(jnp.abs(lower), jnp.exp(-joined))
        hidden_out[:, mine] = (upper / guarded).astype(jnp.bfloat16)


def in_vmem(kernel, outs, *args, limit=12):
    return pl.pallas_call(
        kernel,
        out_shape=[jax.ShapeDtypeStruct(*out) for out in outs],
        compiler_params=pltpu.CompilerParams(vmem_limit_bytes=limit * 1024 * 1024),
    )(*args)


def project_kernel(*refs):
    pieces, weights, others = refs[0], refs[1:5], refs[5:9]
    places, residual, gain, mixed_out, normed_out = refs[9:]
    half = weights[0].shape[1]
    is_first = places[0] == 0
    count = pieces.shape[0]
    shares = []
    for k, offset in enumerate((0, count - 1, 1, 2)):
        piece = pieces[(places[1] + offset) % count]
        low, high = piece[:, :half], piece[:, half:]
        own = jnp.where(is_first, low, high)
        away = jnp.where(is_first, high, low)
        share = lax.dot_general(
            own,
            weights[k][...],
            (((1,), (1,)), ((), ())),
            preferred_element_type=jnp.float32,
        ) + lax.dot_general(
            away,
            others[k][...],
            (((1,), (1,)), ((), ())),
            preferred_element_type=jnp.float32,
        )
        shares.append(share.astype(jnp.bfloat16).astype(jnp.float32))
    projected = sum(shares[1:], shares[0])
    mixed = (residual[...].astype(jnp.float32) + projected).astype(jnp.bfloat16)
    mixed_out[...] = mixed
    mixed = mixed.astype(jnp.float32)
    norm_scale = lax.rsqrt(jnp.mean(mixed * mixed, axis=-1, keepdims=True) + epsilon)
    normed_out[...] = (mixed * norm_scale * gain[...]).astype(jnp.bfloat16)


def projection_weights(own):
    weights = (own, *(shifted(own, "tp", by) for by in (1, -1, 2)))
    others = []
    for piece in weights:
        others.append(shifted(piece, "sp_2", 1))
    return weights, others


def slot_index(ids, experts, capacity):
    flat_ids = ids.reshape(-1)
    matches = (flat_ids[:, None] == jnp.arange(experts, dtype=jnp.int32)[None, :]).astype(jnp.int32)
    before = jnp.cumsum(matches, axis=0) - matches
    return flat_ids * capacity + jnp.sum(before * matches, axis=1)


def slot_masks(own_slots, routed_weight, chunks, experts, capacity):
    masks = []
    for low, high in chunks:
        slots = jnp.arange(experts)[:, None] * capacity + jnp.arange(low, high)[None, :]
        slots = slots.reshape(-1)
        chosen = jnp.zeros((slots.shape[0], own_slots.shape[0]), jnp.bool_)
        weighted = jnp.zeros(chosen.shape, jnp.float32)
        for k in range(own_slots.shape[1]):
            match = slots[:, None] == own_slots[:, k][None, :]
            chosen = chosen | match
            weighted = jnp.where(match, routed_weight[:, k][None, :], weighted)
        masks.append(lax.optimization_barrier((chosen.astype(jnp.bfloat16), weighted)))
    return masks


def local(
    memory_queries,
    memory_keys,
    memory_values,
    input_gate_logits,
    forget_gate_logits,
    extra_log_decay,
    residual,
    cell_output_weight,
    expert_norm_gain,
    expert_gate_weight,
    expert_up_weight,
    expert_down_weight,
    routed_expert_index,
    routed_expert_weight,
):
    f32, bf16 = jnp.float32, jnp.bfloat16
    heads, tokens = input_gate_logits.shape
    channels = memory_keys.shape[1]
    width = channels // heads
    running, mat, norm, final_log, peak = in_vmem(
        summary_kernel,
        (
            ((heads, tokens), f32),
            ((channels, width), f32),
            ((heads, width), f32),
            ((heads, width), f32),
            ((heads, width), f32),
        ),
        memory_keys,
        memory_values,
        input_gate_logits,
        forget_gate_logits,
        extra_log_decay,
        limit=60,
    )
    prior_mat, prior_norm, prior_peak, own_rows = earlier_state(
        final_log[:, 0], mat, norm, peak[:, 0], cell_output_weight
    )
    weights, other_weights = projection_weights(own_rows)
    numer, stats = in_vmem(
        within_kernel,
        (((tokens, channels), f32), ((tokens, 128), f32)),
        memory_queries,
        memory_keys,
        memory_values,
        input_gate_logits,
        running,
    )
    (hidden,) = in_vmem(
        finish_kernel,
        (((tokens, channels), bf16),),
        memory_queries,
        running,
        numer,
        stats,
        prior_mat,
        prior_norm,
        jnp.broadcast_to(prior_peak[:, None], (heads, width)),
    )
    row_count, model_width = residual.shape
    place = lax.axis_index("tp")
    pieces = sent_round(hidden.reshape(-1, row_count, channels), "tp")
    here = pl.BlockSpec()
    mixed_rows, normed = pl.pallas_call(
        project_kernel,
        out_shape=[jax.ShapeDtypeStruct(residual.shape, bf16)] * 2,
        in_specs=[here] * 9 + [pl.BlockSpec(memory_space=pltpu.SMEM)] + [here] * 2,
        compiler_params=pltpu.CompilerParams(vmem_limit_bytes=12 * 1024 * 1024),
        name="project_kernel",
    )(
        pieces,
        *weights,
        *other_weights,
        jnp.stack([lax.axis_index("sp_2"), place]),
        residual,
        expert_norm_gain[None, :],
    )
    mixed_wide = mixed_rows.astype(f32)
    sp_size = lax.axis_size(SP)
    top_count = routed_expert_index.shape[1]
    experts = sp_size * expert_gate_weight.shape[0]
    assigned = row_count * top_count
    capacity = max(2, assigned * 5 // (4 * experts))
    own_ids = lax.dynamic_slice_in_dim(routed_expert_index, place * row_count, row_count, 0)
    chunks = ((0, 2), (2, 5))
    own_slots = slot_index(own_ids, experts, capacity).reshape(row_count, top_count)
    masks = slot_masks(own_slots, routed_expert_weight, chunks, experts, capacity)
    routed_sum = jnp.zeros((row_count, model_width), jnp.float32)
    lane = 128
    sub = model_width // lane
    arrived = []
    for (low, high), (chosen, weighted) in zip(chunks, masks):
        picked = jnp.dot(
            chosen, normed, preferred_element_type=jnp.float32
        ).astype(jnp.bfloat16)
        sent = picked.reshape(experts, (high - low) * sub, lane)
        arrived.append((weighted, sent_round(sent, SP)))
    weights_here = (expert_gate_weight[0], expert_up_weight[0], expert_down_weight[0])
    answers = []
    for weighted, got in arrived:
        rows = got.reshape(-1, model_width)
        half = rows.shape[0] // 2
        number = len(answers)
        blocks = ring_gathered(rows[:half], rows[half:], "tp")
        if number == 0:
            terms = expert_rows(blocks, weights_here, 4)
        else:
            terms = (
                *expert_rows(blocks[:6], weights_here, 2), *expert_rows(blocks[6:], weights_here, 2)
            )
        first, second = ring_summed(terms, "tp")
        summed = jnp.concatenate([first, second], axis=0).astype(jnp.bfloat16)
        returned = sent_round(summed.reshape(got.shape), SP).reshape(-1, model_width)
        answers.append((weighted, returned))
    for weighted, returned in answers:
        routed_sum = routed_sum + lax.dot_general(
            weighted,
            returned.astype(jnp.float32),
            (((0,), (0,)), ((), ())),
            precision=lax.Precision.HIGHEST,
            preferred_element_type=jnp.float32,
        )
    return (mixed_wide + routed_sum).astype(jnp.bfloat16)


def solution(mesh):
    finer = Mesh(mesh.devices.reshape(8, 4, 2, mesh.shape["tp"]), ("sp_0", "sp_1", "sp_2", "tp"))
    placed = (
        P(SP, "tp"),
        P(SP, "tp"),
        P(SP, "tp"),
        P("tp", SP),
        P("tp", SP),
        P("tp", SP),
        P(SP_TP, None),
        P("tp", SP),
        P(),
        P(SP, None, "tp"),
        P(SP, None, "tp"),
        P(SP, "tp", None),
        P(SP, None),
        P(SP_TP, None),
    )
    return jax.shard_map(
        local, mesh=finer, in_specs=placed, out_specs=P(SP_TP, None), check_vma=False
    )
```

```python
import jax
import jax.numpy as jnp
from jax import lax
from jax.experimental import pallas as pl
from jax.experimental.pallas import tpu as pltpu
from jax.sharding import Mesh
from jax.sharding import PartitionSpec as P

SP = ("sp_0", "sp_1", "sp_2")
SP_TP = ("sp_0", "sp_1", "sp_2", "tp")


lowest = -1e30
epsilon = 1e-06


def sent_round(x, axis):
    return lax.all_to_all(x, axis, split_axis=0, concat_axis=0, tiled=True)


def shifted(x, axis, by):
    size = lax.axis_size(axis)
    return lax.ppermute(x, axis, [(i, (i + by) % size) for i in range(size)])


def terms_of(x, count):
    terms = []
    for _ in range(count):
        top = lax.reduce_precision(x, 8, 7)
        terms.append(top.astype(jnp.bfloat16))
        x = x - top
    return terms


def term_sum(x, count):
    parts = jnp.split(x.astype(jnp.float32), count, axis=-1)
    return sum(parts[1:], parts[0])


def side_row(parts, width):
    row = jnp.concatenate([term for part in parts for term in terms_of(part, 3)], axis=1)
    return jnp.pad(row, ((0, 0), (0, width - row.shape[1])))[:, None, :]


def earlier_state(final_log, mat, norm, peak, weight):
    size, heads = lax.axis_size(SP), final_log.shape[0]
    width = mat.shape[-1]
    per_slice = norm.size // size
    spots = jnp.arange(size)
    both = jnp.stack([final_log, peak], axis=1).reshape(1, -1)
    side = side_row(
        [norm.reshape(size, per_slice), jnp.broadcast_to(both, (size, both.shape[1]))], width
    )
    body = mat.reshape(size, -1, width)
    rows = body.shape[1]
    flat = weight.T
    columns = flat.shape[0]
    halves = jnp.stack([flat[:, :width], flat[:, width:]])
    for_all = jnp.broadcast_to(halves, (size // 2, *halves.shape)).reshape(size, columns, width)
    sent = jnp.concatenate([for_all, *terms_of(body, 2), side], axis=1)
    sent = jnp.pad(sent, ((0, 0), (0, -sent.shape[1] % 16), (0, 0)))
    got = sent_round(sent, SP)
    weight_rows = got[:, :columns].reshape(-1, width)
    got_mat = wide(got[:, columns : columns + rows]) + wide(
        got[:, columns + rows : columns + 2 * rows]
    )
    got_side = got[:, columns + 2 * rows]
    got_norm = term_sum(got_side[:, : 3 * per_slice], 3)
    scalars = term_sum(got_side[:, 3 * per_slice : 3 * per_slice + 6 * heads], 3)
    head = lax.axis_index(SP) * heads // size
    lane = jnp.arange(2 * heads)[None, :]
    logs = jnp.sum(jnp.where(lane == 2 * head, scalars, 0.0), axis=1)
    peaks = jnp.sum(jnp.where(lane == 2 * head + 1, scalars, 0.0), axis=1)
    between = (spots[None, None, :] < spots[:, None, None]) & (
        spots[None, None, :] > spots[None, :, None]
    )
    decay = jnp.sum(jnp.where(between, logs[None, None, :], 0.0), axis=-1)
    before = spots[None, :] < spots[:, None]
    level = jnp.where(before, peaks[None, :] + decay, lowest)
    top = jnp.max(level, axis=1)
    scale = jnp.where(before, jnp.exp(level - top[:, None]), 0.0)
    highest = lax.Precision.HIGHEST
    joined_mat = jnp.dot(scale, got_mat.reshape(size, -1), precision=highest)
    joined_norm = jnp.dot(scale, got_norm, precision=highest)
    back = jnp.concatenate(
        [
            joined_mat.reshape(size, rows, width).astype(jnp.bfloat16),
            side_row([joined_norm, top[:, None]], width),
        ],
        axis=1,
    )
    back = jnp.pad(back, ((0, 0), (0, -back.shape[1] % 8), (0, 0)))
    back = sent_round(back, SP)
    prior_mat = back[:, :rows].reshape(mat.shape)
    side = lax.optimization_barrier(back[:, rows])
    prior_norm = term_sum(side[:, : 3 * per_slice], 3).reshape(norm.shape)
    prior_peak = term_sum(side[:: size // heads, 3 * per_slice : 3 * per_slice + 3], 3)[:, 0]
    return prior_mat, prior_norm, prior_peak, weight_rows


def ring_gathered(first, second, axis):
    right_2 = shifted(second, axis, -1)
    left_2 = shifted(second, axis, 1)
    left_1 = shifted(first, axis, 1)
    right_1 = shifted(first, axis, -1)
    far_1 = shifted(left_1, axis, 1)
    far_2 = shifted(right_2, axis, -1)
    return (first, second, left_1, left_2, right_1, right_2, far_1, far_2)


def wide(x):
    return x.astype(jnp.float32)


def ring_summed(blocks, axis):
    own_1, own_2, left_1, left_2, right_1, right_2, far_1, far_2 = blocks
    far_in_1 = shifted(far_1, axis, 1)
    far_in_2 = shifted(far_2, axis, -1)
    from_left_2 = shifted(right_2, axis, 1)
    from_right_1 = shifted(left_1, axis, -1)
    from_left_1 = shifted((wide(right_1) + wide(far_in_1)).astype(jnp.bfloat16), axis, 1)
    from_right_2 = shifted((wide(left_2) + wide(far_in_2)).astype(jnp.bfloat16), axis, -1)
    first = wide(own_1) + wide(from_left_1) + wide(from_right_1)
    second = wide(own_2) + wide(from_left_2) + wide(from_right_2)
    return first, second


def expert_kernel(count, rows, per_tile, loads, *refs):
    given, sources = refs[:count], refs[count : count + 3]
    outs = refs[count + 3 : 2 * count + 3]
    rows_in, rows_out, in_sems, out_sems, weight_sems, *held = refs[2 * count + 3 :]
    gate, up, down = held if loads else sources
    weights = [
        pltpu.make_async_copy(source, weight, weight_sems.at[k])
        for k, (source, weight) in enumerate(zip(sources, held))
    ]
    entries = [
        pltpu.make_async_copy(given[k], rows_in.at[pl.ds(k * rows, rows)], in_sems.at[k])
        for k in range(count)
    ]
    stores = [
        pltpu.make_async_copy(rows_out.at[pl.ds(k * rows, rows)], outs[k], out_sems.at[k])
        for k in range(count)
    ]
    tile = per_tile * rows
    tiles = count // per_tile
    for copy in weights[:1] + entries + weights[1:]:
        copy.start()

    def at_tile(k, action, copies):
        for here in range(tiles):

            @pl.when(k == here)
            def _():
                for copy in copies[here * per_tile : (here + 1) * per_tile]:
                    getattr(copy, action)()

    def one_tile(k, carry):
        here = pl.ds(pl.multiple_of(k * tile, tile), tile)
        at_tile(k, "wait", entries)
        x = rows_in[here, :]
        if loads:
            pl.when(k == 0)(weights[0].wait)
        gate_pre = jnp.dot(x, gate[...], preferred_element_type=jnp.float32)
        if loads:
            pl.when(k == 0)(weights[1].wait)
        up_pre = jnp.dot(x, up[...], preferred_element_type=jnp.float32)
        inner = (gate_pre / (1.0 + jnp.exp(-gate_pre)) * up_pre).astype(jnp.bfloat16)
        if loads:
            pl.when(k == 0)(weights[2].wait)
        rows_out[here, :] = jnp.dot(
            inner, down[...], preferred_element_type=jnp.float32
        ).astype(jnp.bfloat16)
        at_tile(k, "start", stores)
        return carry

    lax.fori_loop(0, tiles, one_tile, 0)
    for store in stores:
        store.wait()


def expert_rows(blocks, weights, per_tile, loads):
    count = len(blocks)
    rows, width = blocks[0].shape
    hidden = weights[0].shape[1]
    anywhere = pl.BlockSpec(memory_space=pl.ANY)
    here = pl.BlockSpec(memory_space=pltpu.VMEM)
    return pl.pallas_call(
        lambda *refs: expert_kernel(count, rows, per_tile, loads, *refs),
        out_shape=[jax.ShapeDtypeStruct((rows, width), jnp.bfloat16)] * count,
        in_specs=[anywhere] * count + [anywhere if loads else here] * 3,
        out_specs=[anywhere] * count,
        scratch_shapes=[
            pltpu.VMEM((count * rows, width), jnp.bfloat16),
            pltpu.VMEM((count * rows, width), jnp.bfloat16),
            pltpu.SemaphoreType.DMA((count,)),
            pltpu.SemaphoreType.DMA((count,)),
            pltpu.SemaphoreType.DMA((3,)),
            *(pltpu.VMEM(w.shape, w.dtype) for w in weights if loads),
        ],
        compiler_params=pltpu.CompilerParams(
            vmem_limit_bytes=(46 if loads else 28) * 1024 * 1024
        ),
        cost_estimate=pl.CostEstimate(
            flops=6 * count * rows * width * hidden,
            transcendentals=count * rows * hidden,
            bytes_accessed=6 * width * hidden + 4 * count * rows * width,
        ),
    )(*blocks, *weights)


def column(row, lanes=128):
    return jnp.transpose(jnp.broadcast_to(row, (lanes, row.shape[1])))


def summary_kernel(
    keys, values, gate_in, forget, extra, running_out, mat_out, norm_out, log_out, peak_out
):
    heads, length = gate_in.shape
    width = keys.shape[1] // heads
    raw = forget[...]
    running = jnp.minimum(raw, 0.0) - jnp.log1p(jnp.exp(-jnp.abs(raw))) + extra[...]
    lane = lax.broadcasted_iota(jnp.int32, running.shape, 1)
    step = 1
    while step < length:
        running = running + jnp.where(lane >= step, pltpu.roll(running, step, 1), 0.0)
        step *= 2
    running_out[...] = running
    final = running[:, length - 1 :]
    keep = final - running + gate_in[...]
    peak = jnp.max(keep, axis=1, keepdims=True)
    retain = jnp.exp(keep - peak)
    log_out[...] = jnp.broadcast_to(final, log_out.shape)
    peak_out[...] = jnp.broadcast_to(peak, peak_out.shape)
    for h in range(heads):
        mine = pl.ds(h * width, width)
        key = keys[:, mine]
        row = retain[h : h + 1]
        scaled = (column(row) * values[:, mine].astype(jnp.float32)).astype(jnp.bfloat16)
        mat_out[mine, :] = lax.dot_general(
            scaled, key, (((0,), (0,)), ((), ())), preferred_element_type=jnp.float32
        )
        norm_out[pl.ds(h, 1), :] = jnp.sum(
            column(row) * key.astype(jnp.float32), axis=0, keepdims=True
        )


def within_kernel(queries, keys, values, gate_in, running, numer_out, stats_out):
    heads, length = gate_in.shape
    width = keys.shape[1] // heads
    scale = width ** (-0.5)
    times = lax.broadcasted_iota(jnp.int32, (length, length), 0)
    sources = lax.broadcasted_iota(jnp.int32, (length, length), 1)
    causal = times >= sources
    place = lax.broadcasted_iota(jnp.int32, stats_out.shape, 1)
    stats = jnp.zeros(stats_out.shape, jnp.float32)
    for h in range(heads):
        mine = pl.ds(h * width, width)
        row = running[h : h + 1, :]
        down = column(row)[:, :1]
        level = jnp.where(causal, down - row + gate_in[h : h + 1, :], -jnp.inf)
        top = jnp.max(level, axis=1, keepdims=True)
        match = lax.dot_general(
            queries[:, mine],
            keys[:, mine],
            (((1,), (1,)), ((), ())),
            preferred_element_type=jnp.float32,
        )
        share = jnp.exp(level - top) * (match * scale)
        numer_out[:, mine] = jnp.dot(
            share.astype(jnp.bfloat16), values[:, mine], preferred_element_type=jnp.float32
        )
        total = jnp.sum(share, axis=1, keepdims=True)
        stats = jnp.where(place == 2 * h, total, stats)
        stats = jnp.where(place == 2 * h + 1, top, stats)
    stats_out[...] = stats


def finish_kernel(queries, running, numer, stats, mat, norm, peak, hidden_out):
    heads = running.shape[0]
    width = queries.shape[1] // heads
    scale = width ** (-0.5)
    for h in range(heads):
        mine = pl.ds(h * width, width)
        reached = column(running[h : h + 1, :])[:, :1] + peak[h : h + 1, :1]
        total = stats[:, 2 * h : 2 * h + 1]
        top = stats[:, 2 * h + 1 : 2 * h + 2]
        joined = jnp.maximum(top, reached)
        near = jnp.exp(top - joined)
        far = jnp.exp(reached - joined)
        query = queries[:, mine]
        past = lax.dot_general(
            query,
            mat[mine, :],
            (((1,), (1,)), ((), ())),
            preferred_element_type=jnp.float32,
        )
        past_total = jnp.sum(
            query.astype(jnp.float32) * norm[h : h + 1, :], axis=1, keepdims=True
        )
        upper = near * numer[:, mine] + far * (past * scale)
        lower = near * total + far * (past_total * scale)
        guarded = jnp.maximum(jnp.abs(lower), jnp.exp(-joined))
        hidden_out[:, mine] = (upper / guarded).astype(jnp.bfloat16)


def in_vmem(kernel, outs, *args, limit=12):
    return pl.pallas_call(
        kernel,
        out_shape=[jax.ShapeDtypeStruct(*out) for out in outs],
        compiler_params=pltpu.CompilerParams(vmem_limit_bytes=limit * 1024 * 1024),
    )(*args)


def project_kernel(*refs):
    pieces, weights, others = refs[0], refs[1:5], refs[5:9]
    places, residual, gain, mixed_out, normed_out = refs[9:]
    half = weights[0].shape[1]
    is_first = places[0] == 0
    count = pieces.shape[0]
    shares = []
    for k, offset in enumerate((0, count - 1, 1, 2)):
        piece = pieces[(places[1] + offset) % count]
        low, high = piece[:, :half], piece[:, half:]
        own = jnp.where(is_first, low, high)
        away = jnp.where(is_first, high, low)
        share = lax.dot_general(
            own,
            weights[k][...],
            (((1,), (1,)), ((), ())),
            preferred_element_type=jnp.float32,
        ) + lax.dot_general(
            away,
            others[k][...],
            (((1,), (1,)), ((), ())),
            preferred_element_type=jnp.float32,
        )
        shares.append(share.astype(jnp.bfloat16).astype(jnp.float32))
    projected = sum(shares[1:], shares[0])
    mixed = (residual[...].astype(jnp.float32) + projected).astype(jnp.bfloat16)
    mixed_out[...] = mixed
    mixed = mixed.astype(jnp.float32)
    norm_scale = lax.rsqrt(jnp.mean(mixed * mixed, axis=-1, keepdims=True) + epsilon)
    normed_out[...] = (mixed * norm_scale * gain[...]).astype(jnp.bfloat16)


def projection_weights(own):
    weights = (own, *(shifted(own, "tp", by) for by in (1, -1, 2)))
    others = []
    for piece in weights:
        others.append(shifted(piece, "sp_2", 1))
    return weights, others


def slot_index(ids, experts, capacity):
    flat_ids = ids.reshape(-1)
    matches = (flat_ids[:, None] == jnp.arange(experts, dtype=jnp.int32)[None, :]).astype(jnp.int32)
    before = jnp.cumsum(matches, axis=0) - matches
    return flat_ids * capacity + jnp.sum(before * matches, axis=1)


def slot_masks(own_slots, routed_weight, chunks, experts, capacity):
    masks = []
    for low, high in chunks:
        slots = jnp.arange(experts)[:, None] * capacity + jnp.arange(low, high)[None, :]
        slots = slots.reshape(-1)
        chosen = jnp.zeros((slots.shape[0], own_slots.shape[0]), jnp.bool_)
        weighted = jnp.zeros(chosen.shape, jnp.float32)
        for k in range(own_slots.shape[1]):
            match = slots[:, None] == own_slots[:, k][None, :]
            chosen = chosen | match
            weighted = jnp.where(match, routed_weight[:, k][None, :], weighted)
        masks.append(lax.optimization_barrier((chosen.astype(jnp.bfloat16), weighted)))
    return masks


def local(
    memory_queries,
    memory_keys,
    memory_values,
    input_gate_logits,
    forget_gate_logits,
    extra_log_decay,
    residual,
    cell_output_weight,
    expert_norm_gain,
    expert_gate_weight,
    expert_up_weight,
    expert_down_weight,
    routed_expert_index,
    routed_expert_weight,
):
    f32, bf16 = jnp.float32, jnp.bfloat16
    heads, tokens = input_gate_logits.shape
    channels = memory_keys.shape[1]
    width = channels // heads
    running, mat, norm, final_log, peak = in_vmem(
        summary_kernel,
        (
            ((heads, tokens), f32),
            ((channels, width), f32),
            ((heads, width), f32),
            ((heads, width), f32),
            ((heads, width), f32),
        ),
        memory_keys,
        memory_values,
        input_gate_logits,
        forget_gate_logits,
        extra_log_decay,
        limit=60,
    )
    prior_mat, prior_norm, prior_peak, own_rows = earlier_state(
        final_log[:, 0], mat, norm, peak[:, 0], cell_output_weight
    )
    weights, other_weights = projection_weights(own_rows)
    numer, stats = in_vmem(
        within_kernel,
        (((tokens, channels), f32), ((tokens, 128), f32)),
        memory_queries,
        memory_keys,
        memory_values,
        input_gate_logits,
        running,
        limit=60,
    )
    (hidden,) = in_vmem(
        finish_kernel,
        (((tokens, channels), bf16),),
        memory_queries,
        running,
        numer,
        stats,
        prior_mat,
        prior_norm,
        jnp.broadcast_to(prior_peak[:, None], (heads, width)),
        limit=60,
    )
    row_count, model_width = residual.shape
    place = lax.axis_index("tp")
    pieces = sent_round(hidden.reshape(-1, row_count, channels), "tp")
    here = pl.BlockSpec()
    mixed_rows, normed = pl.pallas_call(
        project_kernel,
        out_shape=[jax.ShapeDtypeStruct(residual.shape, bf16)] * 2,
        in_specs=[here] * 9 + [pl.BlockSpec(memory_space=pltpu.SMEM)] + [here] * 2,
        compiler_params=pltpu.CompilerParams(vmem_limit_bytes=12 * 1024 * 1024),
        name="project_kernel",
    )(
        pieces,
        *weights,
        *other_weights,
        jnp.stack([lax.axis_index("sp_2"), place]),
        residual,
        expert_norm_gain[None, :],
    )
    mixed_wide = mixed_rows.astype(f32)
    sp_size = lax.axis_size(SP)
    top_count = routed_expert_index.shape[1]
    experts = sp_size * expert_gate_weight.shape[0]
    assigned = row_count * top_count
    capacity = max(2, assigned * 5 // (4 * experts))
    own_ids = lax.dynamic_slice_in_dim(routed_expert_index, place * row_count, row_count, 0)
    chunks = ((0, 2), (2, 5))
    own_slots = slot_index(own_ids, experts, capacity).reshape(row_count, top_count)
    masks = slot_masks(own_slots, routed_expert_weight, chunks, experts, capacity)
    routed_sum = jnp.zeros((row_count, model_width), jnp.float32)
    lane = 128
    sub = model_width // lane
    arrived = []
    for (low, high), (chosen, weighted) in zip(chunks, masks):
        picked = jnp.dot(
            chosen, normed, preferred_element_type=jnp.float32
        ).astype(jnp.bfloat16)
        sent = picked.reshape(experts, (high - low) * sub, lane)
        arrived.append((weighted, sent_round(sent, SP)))
    weights_here = (expert_gate_weight[0], expert_up_weight[0], expert_down_weight[0])
    answers = []
    for weighted, got in arrived:
        rows = got.reshape(-1, model_width)
        half = rows.shape[0] // 2
        number = len(answers)
        blocks = ring_gathered(rows[:half], rows[half:], "tp")
        if number == 0:
            terms = expert_rows(blocks, weights_here, 4, True)
        else:
            terms = (
                *expert_rows(blocks[:6], weights_here, 2, False),
                *expert_rows(blocks[6:], weights_here, 2, False),
            )
        first, second = ring_summed(terms, "tp")
        summed = jnp.concatenate([first, second], axis=0).astype(jnp.bfloat16)
        returned = sent_round(summed.reshape(got.shape), SP).reshape(-1, model_width)
        answers.append((weighted, returned))
    for weighted, returned in answers:
        routed_sum = routed_sum + lax.dot_general(
            weighted,
            returned.astype(jnp.float32),
            (((0,), (0,)), ((), ())),
            precision=lax.Precision.HIGHEST,
            preferred_element_type=jnp.float32,
        )
    return (mixed_wide + routed_sum).astype(jnp.bfloat16)


def solution(mesh):
    finer = Mesh(mesh.devices.reshape(8, 4, 2, mesh.shape["tp"]), ("sp_0", "sp_1", "sp_2", "tp"))
    placed = (
        P(SP, "tp"),
        P(SP, "tp"),
        P(SP, "tp"),
        P("tp", SP),
        P("tp", SP),
        P("tp", SP),
        P(SP_TP, None),
        P("tp", SP),
        P(),
        P(SP, None, "tp"),
        P(SP, None, "tp"),
        P(SP, "tp", None),
        P(SP, None),
        P(SP_TP, None),
    )
    return jax.shard_map(
        local, mesh=finer, in_specs=placed, out_specs=P(SP_TP, None), check_vma=False
    )
```

```python
import jax
import jax.numpy as jnp
from jax import lax
from jax.experimental import pallas as pl
from jax.experimental.pallas import tpu as pltpu
from jax.sharding import Mesh
from jax.sharding import PartitionSpec as P

SP = ("sp_0", "sp_1", "sp_2")
SP_TP = ("sp_0", "sp_1", "sp_2", "tp")


lowest = -1e30
epsilon = 1e-06


def sent_round(x, axis):
    return lax.all_to_all(x, axis, split_axis=0, concat_axis=0, tiled=True)


def shifted(x, axis, by):
    size = lax.axis_size(axis)
    return lax.ppermute(x, axis, [(i, (i + by) % size) for i in range(size)])


def terms_of(x, count):
    terms = []
    for _ in range(count):
        top = lax.reduce_precision(x, 8, 7)
        terms.append(top.astype(jnp.bfloat16))
        x = x - top
    return terms


def term_sum(x, count):
    parts = jnp.split(x.astype(jnp.float32), count, axis=-1)
    return sum(parts[1:], parts[0])


def side_row(parts, width):
    row = jnp.concatenate([term for part in parts for term in terms_of(part, 3)], axis=1)
    return jnp.pad(row, ((0, 0), (0, width - row.shape[1])))[:, None, :]


def earlier_state(final_log, mat, norm, peak, weight):
    size, heads = lax.axis_size(SP), final_log.shape[0]
    width = mat.shape[-1]
    per_slice = norm.size // size
    spots = jnp.arange(size)
    both = jnp.stack([final_log, peak], axis=1).reshape(1, -1)
    side = side_row(
        [norm.reshape(size, per_slice), jnp.broadcast_to(both, (size, both.shape[1]))], width
    )
    body = mat.reshape(size, -1, width)
    rows = body.shape[1]
    flat = weight.T
    columns = flat.shape[0]
    halves = jnp.stack([flat[:, :width], flat[:, width:]])
    for_all = jnp.broadcast_to(halves, (size // 2, *halves.shape)).reshape(size, columns, width)
    sent = jnp.concatenate([for_all, body.astype(jnp.bfloat16), side], axis=1)
    sent = jnp.pad(sent, ((0, 0), (0, -sent.shape[1] % 8), (0, 0)))
    got = sent_round(sent, SP)
    weight_rows = got[:, :columns].reshape(-1, width)
    got_mat = wide(got[:, columns : columns + rows])
    got_side = got[:, columns + rows]
    got_norm = term_sum(got_side[:, : 3 * per_slice], 3)
    scalars = term_sum(got_side[:, 3 * per_slice : 3 * per_slice + 6 * heads], 3)
    head = lax.axis_index(SP) * heads // size
    lane = jnp.arange(2 * heads)[None, :]
    logs = jnp.sum(jnp.where(lane == 2 * head, scalars, 0.0), axis=1)
    peaks = jnp.sum(jnp.where(lane == 2 * head + 1, scalars, 0.0), axis=1)
    between = (spots[None, None, :] < spots[:, None, None]) & (
        spots[None, None, :] > spots[None, :, None]
    )
    decay = jnp.sum(jnp.where(between, logs[None, None, :], 0.0), axis=-1)
    before = spots[None, :] < spots[:, None]
    level = jnp.where(before, peaks[None, :] + decay, lowest)
    top = jnp.max(level, axis=1)
    scale = jnp.where(before, jnp.exp(level - top[:, None]), 0.0)
    highest = lax.Precision.HIGHEST
    joined_mat = jnp.dot(scale, got_mat.reshape(size, -1), precision=highest)
    joined_norm = jnp.dot(scale, got_norm, precision=highest)
    back = jnp.concatenate(
        [
            joined_mat.reshape(size, rows, width).astype(jnp.bfloat16),
            side_row([joined_norm, top[:, None]], width),
        ],
        axis=1,
    )
    back = jnp.pad(back, ((0, 0), (0, -back.shape[1] % 8), (0, 0)))
    back = sent_round(back, SP)
    prior_mat = back[:, :rows].reshape(mat.shape)
    side = lax.optimization_barrier(back[:, rows])
    prior_norm = term_sum(side[:, : 3 * per_slice], 3).reshape(norm.shape)
    prior_peak = term_sum(side[:: size // heads, 3 * per_slice : 3 * per_slice + 3], 3)[:, 0]
    return prior_mat, prior_norm, prior_peak, weight_rows


def ring_gathered(first, second, axis):
    right_2 = shifted(second, axis, -1)
    left_2 = shifted(second, axis, 1)
    left_1 = shifted(first, axis, 1)
    right_1 = shifted(first, axis, -1)
    far_1 = shifted(left_1, axis, 1)
    far_2 = shifted(right_2, axis, -1)
    return (first, second, left_1, left_2, right_1, right_2, far_1, far_2)


def wide(x):
    return x.astype(jnp.float32)


def ring_summed(blocks, axis):
    own_1, own_2, left_1, left_2, right_1, right_2, far_1, far_2 = blocks
    far_in_1 = shifted(far_1, axis, 1)
    far_in_2 = shifted(far_2, axis, -1)
    from_left_2 = shifted(right_2, axis, 1)
    from_right_1 = shifted(left_1, axis, -1)
    from_left_1 = shifted((wide(right_1) + wide(far_in_1)).astype(jnp.bfloat16), axis, 1)
    from_right_2 = shifted((wide(left_2) + wide(far_in_2)).astype(jnp.bfloat16), axis, -1)
    first = wide(own_1) + wide(from_left_1) + wide(from_right_1)
    second = wide(own_2) + wide(from_left_2) + wide(from_right_2)
    return first, second


def expert_kernel(count, rows, per_tile, loads, *refs):
    given, sources = refs[:count], refs[count : count + 3]
    outs = refs[count + 3 : 2 * count + 3]
    rows_in, rows_out, in_sems, out_sems, weight_sems, *held = refs[2 * count + 3 :]
    gate, up, down = held if loads else sources
    weights = [
        pltpu.make_async_copy(source, weight, weight_sems.at[k])
        for k, (source, weight) in enumerate(zip(sources, held))
    ]
    entries = [
        pltpu.make_async_copy(given[k], rows_in.at[pl.ds(k * rows, rows)], in_sems.at[k])
        for k in range(count)
    ]
    stores = [
        pltpu.make_async_copy(rows_out.at[pl.ds(k * rows, rows)], outs[k], out_sems.at[k])
        for k in range(count)
    ]
    tile = per_tile * rows
    tiles = count // per_tile
    for copy in weights[:1] + entries + weights[1:]:
        copy.start()

    def at_tile(k, action, copies):
        for here in range(tiles):

            @pl.when(k == here)
            def _():
                for copy in copies[here * per_tile : (here + 1) * per_tile]:
                    getattr(copy, action)()

    def one_tile(k, carry):
        here = pl.ds(pl.multiple_of(k * tile, tile), tile)
        at_tile(k, "wait", entries)
        x = rows_in[here, :]
        if loads:
            pl.when(k == 0)(weights[0].wait)
        gate_pre = jnp.dot(x, gate[...], preferred_element_type=jnp.float32)
        if loads:
            pl.when(k == 0)(weights[1].wait)
        up_pre = jnp.dot(x, up[...], preferred_element_type=jnp.float32)
        inner = (gate_pre / (1.0 + jnp.exp(-gate_pre)) * up_pre).astype(jnp.bfloat16)
        if loads:
            pl.when(k == 0)(weights[2].wait)
        rows_out[here, :] = jnp.dot(
            inner, down[...], preferred_element_type=jnp.float32
        ).astype(jnp.bfloat16)
        at_tile(k, "start", stores)
        return carry

    lax.fori_loop(0, tiles, one_tile, 0)
    for store in stores:
        store.wait()


def expert_rows(blocks, weights, per_tile, loads):
    count = len(blocks)
    rows, width = blocks[0].shape
    hidden = weights[0].shape[1]
    anywhere = pl.BlockSpec(memory_space=pl.ANY)
    here = pl.BlockSpec(memory_space=pltpu.VMEM)
    return pl.pallas_call(
        lambda *refs: expert_kernel(count, rows, per_tile, loads, *refs),
        out_shape=[jax.ShapeDtypeStruct((rows, width), jnp.bfloat16)] * count,
        in_specs=[anywhere] * count + [anywhere if loads else here] * 3,
        out_specs=[anywhere] * count,
        scratch_shapes=[
            pltpu.VMEM((count * rows, width), jnp.bfloat16),
            pltpu.VMEM((count * rows, width), jnp.bfloat16),
            pltpu.SemaphoreType.DMA((count,)),
            pltpu.SemaphoreType.DMA((count,)),
            pltpu.SemaphoreType.DMA((3,)),
            *(pltpu.VMEM(w.shape, w.dtype) for w in weights if loads),
        ],
        compiler_params=pltpu.CompilerParams(
            vmem_limit_bytes=(46 if loads else 28) * 1024 * 1024
        ),
        cost_estimate=pl.CostEstimate(
            flops=6 * count * rows * width * hidden,
            transcendentals=count * rows * hidden,
            bytes_accessed=6 * width * hidden + 4 * count * rows * width,
        ),
    )(*blocks, *weights)


def column(row, lanes=128):
    return jnp.transpose(jnp.broadcast_to(row, (lanes, row.shape[1])))


def summary_kernel(
    keys, values, gate_in, forget, extra, running_out, mat_out, norm_out, log_out, peak_out
):
    heads, length = gate_in.shape
    width = keys.shape[1] // heads
    raw = forget[...]
    running = jnp.minimum(raw, 0.0) - jnp.log1p(jnp.exp(-jnp.abs(raw))) + extra[...]
    lane = lax.broadcasted_iota(jnp.int32, running.shape, 1)
    step = 1
    while step < length:
        running = running + jnp.where(lane >= step, pltpu.roll(running, step, 1), 0.0)
        step *= 2
    running_out[...] = running
    final = running[:, length - 1 :]
    keep = final - running + gate_in[...]
    peak = jnp.max(keep, axis=1, keepdims=True)
    retain = jnp.exp(keep - peak)
    log_out[...] = jnp.broadcast_to(final, log_out.shape)
    peak_out[...] = jnp.broadcast_to(peak, peak_out.shape)
    for h in range(heads):
        mine = pl.ds(h * width, width)
        key = keys[:, mine]
        row = retain[h : h + 1]
        scaled = (column(row) * values[:, mine].astype(jnp.float32)).astype(jnp.bfloat16)
        mat_out[mine, :] = lax.dot_general(
            scaled, key, (((0,), (0,)), ((), ())), preferred_element_type=jnp.float32
        )
        norm_out[pl.ds(h, 1), :] = jnp.sum(
            column(row) * key.astype(jnp.float32), axis=0, keepdims=True
        )


def within_kernel(queries, keys, values, gate_in, running, numer_out, stats_out):
    heads, length = gate_in.shape
    width = keys.shape[1] // heads
    scale = width ** (-0.5)
    times = lax.broadcasted_iota(jnp.int32, (length, length), 0)
    sources = lax.broadcasted_iota(jnp.int32, (length, length), 1)
    causal = times >= sources
    place = lax.broadcasted_iota(jnp.int32, stats_out.shape, 1)
    stats = jnp.zeros(stats_out.shape, jnp.float32)
    for h in range(heads):
        mine = pl.ds(h * width, width)
        row = running[h : h + 1, :]
        down = column(row)[:, :1]
        level = jnp.where(causal, down - row + gate_in[h : h + 1, :], -jnp.inf)
        top = jnp.max(level, axis=1, keepdims=True)
        match = lax.dot_general(
            queries[:, mine],
            keys[:, mine],
            (((1,), (1,)), ((), ())),
            preferred_element_type=jnp.float32,
        )
        share = jnp.exp(level - top) * (match * scale)
        numer_out[:, mine] = jnp.dot(
            share.astype(jnp.bfloat16), values[:, mine], preferred_element_type=jnp.float32
        )
        total = jnp.sum(share, axis=1, keepdims=True)
        stats = jnp.where(place == 2 * h, total, stats)
        stats = jnp.where(place == 2 * h + 1, top, stats)
    stats_out[...] = stats


def finish_kernel(queries, running, numer, stats, mat, norm, peak, hidden_out):
    heads = running.shape[0]
    width = queries.shape[1] // heads
    scale = width ** (-0.5)
    for h in range(heads):
        mine = pl.ds(h * width, width)
        reached = column(running[h : h + 1, :])[:, :1] + peak[h : h + 1, :1]
        total = stats[:, 2 * h : 2 * h + 1]
        top = stats[:, 2 * h + 1 : 2 * h + 2]
        joined = jnp.maximum(top, reached)
        near = jnp.exp(top - joined)
        far = jnp.exp(reached - joined)
        query = queries[:, mine]
        past = lax.dot_general(
            query,
            mat[mine, :],
            (((1,), (1,)), ((), ())),
            preferred_element_type=jnp.float32,
        )
        past_total = jnp.sum(
            query.astype(jnp.float32) * norm[h : h + 1, :], axis=1, keepdims=True
        )
        upper = near * numer[:, mine] + far * (past * scale)
        lower = near * total + far * (past_total * scale)
        guarded = jnp.maximum(jnp.abs(lower), jnp.exp(-joined))
        hidden_out[:, mine] = (upper / guarded).astype(jnp.bfloat16)


def in_vmem(kernel, outs, *args, limit=12):
    return pl.pallas_call(
        kernel,
        out_shape=[jax.ShapeDtypeStruct(*out) for out in outs],
        compiler_params=pltpu.CompilerParams(vmem_limit_bytes=limit * 1024 * 1024),
    )(*args)


def project_kernel(*refs):
    pieces, weights, others = refs[0], refs[1:5], refs[5:9]
    places, residual, gain, mixed_out, normed_out = refs[9:]
    half = weights[0].shape[1]
    is_first = places[0] == 0
    count = pieces.shape[0]
    shares = []
    for k, offset in enumerate((0, count - 1, 1, 2)):
        piece = pieces[(places[1] + offset) % count]
        low, high = piece[:, :half], piece[:, half:]
        own = jnp.where(is_first, low, high)
        away = jnp.where(is_first, high, low)
        share = lax.dot_general(
            own,
            weights[k][...],
            (((1,), (1,)), ((), ())),
            preferred_element_type=jnp.float32,
        ) + lax.dot_general(
            away,
            others[k][...],
            (((1,), (1,)), ((), ())),
            preferred_element_type=jnp.float32,
        )
        shares.append(share.astype(jnp.bfloat16).astype(jnp.float32))
    projected = sum(shares[1:], shares[0])
    mixed = (residual[...].astype(jnp.float32) + projected).astype(jnp.bfloat16)
    mixed_out[...] = mixed
    mixed = mixed.astype(jnp.float32)
    norm_scale = lax.rsqrt(jnp.mean(mixed * mixed, axis=-1, keepdims=True) + epsilon)
    normed_out[...] = (mixed * norm_scale * gain[...]).astype(jnp.bfloat16)


def projection_weights(own):
    weights = (own, *(shifted(own, "tp", by) for by in (1, -1, 2)))
    others = []
    for piece in weights:
        others.append(shifted(piece, "sp_2", 1))
    return weights, others


def slot_index(ids, experts, capacity):
    flat_ids = ids.reshape(-1)
    matches = (flat_ids[:, None] == jnp.arange(experts, dtype=jnp.int32)[None, :]).astype(jnp.int32)
    before = jnp.cumsum(matches, axis=0) - matches
    return flat_ids * capacity + jnp.sum(before * matches, axis=1)


def slot_masks(own_slots, routed_weight, chunks, experts, capacity):
    masks = []
    for low, high in chunks:
        slots = jnp.arange(experts)[:, None] * capacity + jnp.arange(low, high)[None, :]
        slots = slots.reshape(-1)
        chosen = jnp.zeros((slots.shape[0], own_slots.shape[0]), jnp.bool_)
        weighted = jnp.zeros(chosen.shape, jnp.float32)
        for k in range(own_slots.shape[1]):
            match = slots[:, None] == own_slots[:, k][None, :]
            chosen = chosen | match
            weighted = jnp.where(match, routed_weight[:, k][None, :], weighted)
        masks.append(lax.optimization_barrier((chosen.astype(jnp.bfloat16), weighted)))
    return masks


def local(
    memory_queries,
    memory_keys,
    memory_values,
    input_gate_logits,
    forget_gate_logits,
    extra_log_decay,
    residual,
    cell_output_weight,
    expert_norm_gain,
    expert_gate_weight,
    expert_up_weight,
    expert_down_weight,
    routed_expert_index,
    routed_expert_weight,
):
    f32, bf16 = jnp.float32, jnp.bfloat16
    heads, tokens = input_gate_logits.shape
    channels = memory_keys.shape[1]
    width = channels // heads
    running, mat, norm, final_log, peak = in_vmem(
        summary_kernel,
        (
            ((heads, tokens), f32),
            ((channels, width), f32),
            ((heads, width), f32),
            ((heads, width), f32),
            ((heads, width), f32),
        ),
        memory_keys,
        memory_values,
        input_gate_logits,
        forget_gate_logits,
        extra_log_decay,
        limit=60,
    )
    prior_mat, prior_norm, prior_peak, own_rows = earlier_state(
        final_log[:, 0], mat, norm, peak[:, 0], cell_output_weight
    )
    weights, other_weights = projection_weights(own_rows)
    numer, stats = in_vmem(
        within_kernel,
        (((tokens, channels), f32), ((tokens, 128), f32)),
        memory_queries,
        memory_keys,
        memory_values,
        input_gate_logits,
        running,
    )
    (hidden,) = in_vmem(
        finish_kernel,
        (((tokens, channels), bf16),),
        memory_queries,
        running,
        numer,
        stats,
        prior_mat,
        prior_norm,
        jnp.broadcast_to(prior_peak[:, None], (heads, width)),
    )
    row_count, model_width = residual.shape
    place = lax.axis_index("tp")
    pieces = sent_round(hidden.reshape(-1, row_count, channels), "tp")
    here = pl.BlockSpec()
    mixed_rows, normed = pl.pallas_call(
        project_kernel,
        out_shape=[jax.ShapeDtypeStruct(residual.shape, bf16)] * 2,
        in_specs=[here] * 9 + [pl.BlockSpec(memory_space=pltpu.SMEM)] + [here] * 2,
        compiler_params=pltpu.CompilerParams(vmem_limit_bytes=12 * 1024 * 1024),
        name="project_kernel",
    )(
        pieces,
        *weights,
        *other_weights,
        jnp.stack([lax.axis_index("sp_2"), place]),
        residual,
        expert_norm_gain[None, :],
    )
    mixed_wide = mixed_rows.astype(f32)
    sp_size = lax.axis_size(SP)
    top_count = routed_expert_index.shape[1]
    experts = sp_size * expert_gate_weight.shape[0]
    assigned = row_count * top_count
    capacity = max(2, assigned * 5 // (4 * experts))
    own_ids = lax.dynamic_slice_in_dim(routed_expert_index, place * row_count, row_count, 0)
    chunks = ((0, 2), (2, 5))
    own_slots = slot_index(own_ids, experts, capacity).reshape(row_count, top_count)
    masks = slot_masks(own_slots, routed_expert_weight, chunks, experts, capacity)
    routed_sum = jnp.zeros((row_count, model_width), jnp.float32)
    lane = 128
    sub = model_width // lane
    arrived = []
    for (low, high), (chosen, weighted) in zip(chunks, masks):
        picked = jnp.dot(
            chosen, normed, preferred_element_type=jnp.float32
        ).astype(jnp.bfloat16)
        sent = picked.reshape(experts, (high - low) * sub, lane)
        arrived.append((weighted, sent_round(sent, SP)))
    weights_here = (expert_gate_weight[0], expert_up_weight[0], expert_down_weight[0])
    answers = []
    for weighted, got in arrived:
        rows = got.reshape(-1, model_width)
        half = rows.shape[0] // 2
        number = len(answers)
        blocks = ring_gathered(rows[:half], rows[half:], "tp")
        if number == 0:
            terms = expert_rows(blocks, weights_here, 4, True)
        else:
            terms = (
                *expert_rows(blocks[:6], weights_here, 2, False),
                *expert_rows(blocks[6:], weights_here, 2, False),
            )
        first, second = ring_summed(terms, "tp")
        summed = jnp.concatenate([first, second], axis=0).astype(jnp.bfloat16)
        returned = sent_round(summed.reshape(got.shape), SP).reshape(-1, model_width)
        answers.append((weighted, returned))
    for weighted, returned in answers:
        routed_sum = routed_sum + lax.dot_general(
            weighted,
            returned.astype(jnp.float32),
            (((0,), (0,)), ((), ())),
            precision=lax.Precision.HIGHEST,
            preferred_element_type=jnp.float32,
        )
    return (mixed_wide + routed_sum).astype(jnp.bfloat16)


def solution(mesh):
    finer = Mesh(mesh.devices.reshape(8, 4, 2, mesh.shape["tp"]), ("sp_0", "sp_1", "sp_2", "tp"))
    placed = (
        P(SP, "tp"),
        P(SP, "tp"),
        P(SP, "tp"),
        P("tp", SP),
        P("tp", SP),
        P("tp", SP),
        P(SP_TP, None),
        P("tp", SP),
        P(),
        P(SP, None, "tp"),
        P(SP, None, "tp"),
        P(SP, "tp", None),
        P(SP, None),
        P(SP_TP, None),
    )
    return jax.shard_map(
        local, mesh=finer, in_specs=placed, out_specs=P(SP_TP, None), check_vma=False
    )
```
